32 devices in a mesh: grp: 2 (over y), fs: 4 (over z), tp: 4 (over x, core).
Axes of the slice: x: 2, y: 2, z: 4, core: 2. Of those that a mesh axis runs over, the one named last changes fastest.
Arguments:
- tokens: bfloat16 [1792, 2048], P(('grp', 'fs'), 'tp'), parts along dimension 0, may hold values from -6 to 6
- route_ids: int32 [1792, 2], P(('grp', 'fs')), parts along dimension 0, may hold values from 0 to 3, all different within a row; in each aligned block of 224 rows (0 to 223, 224 to 447, ...) at most 168 rows name the same one
- route_weights: float32 [1792, 2], P(('grp', 'fs')), parts along dimension 0, may hold values from 0.25 to 1
- norm_gain: float32 [2048], P('fs'), may hold values from 0.1 to 1.9
- gate_master: float32 [4, 2048, 512], P(None, 'fs', 'tp'), may hold values from -0.125 to 0.125
- up_master: float32 [4, 2048, 512], P(None, 'fs', 'tp'), may hold values from -0.125 to 0.125
- down_master: float32 [4, 2048, 512], P(None, 'fs', 'tp'), may hold values from -0.25 to 0.25
Outputs:
- gate_serve: bfloat16 [8, 2048, 512], P(('grp', 'fs'), None, 'tp'), parts along dimension 0
- up_serve: bfloat16 [8, 2048, 512], P(('grp', 'fs'), None, 'tp'), parts along dimension 0
- down_serve: bfloat16 [8, 2048, 512], P(('grp', 'fs'), None, 'tp'), parts along dimension 0
- moe_output: bfloat16 [1792, 2048], P(('grp', 'fs'), 'tp'), parts along dimension 0
The draws below stay inside these ranges and needn't reach their ends.
There are 2 independent parts, one for each index of `grp`. The reference program is written for one: setup_inputs(seed, part) draws one part's arguments, and reference() takes and returns one part's arrays. A program takes and returns all parts, laid end to end along the dimension named above; an argument that names none is the same for every part. Nothing has to cross between parts.
Inputs may be any that keep to these rules, and one draw needn't show every extreme that they name: `route_ids`: the 2 experts of a row differ; within the rows of one index of fs (aligned blocks of 224 rows) no expert is named more than 168 times.
All inputs are finite; a program needn't handle non-finite values.
Results may differ from the reference program's by a relative error of at most 0.012.
Values may be sent and summed in bfloat16 or wider, within the bound.
A program may use at most 64 MiB of HBM per device.

```python
import math
import jax
import jax.numpy as jnp
import numpy as np
from jax import lax

D = 2048
F = 512
TOP = 2
TOK_DEV = 224
EXPERTS = 4
TOKENS = 896
CAP = 168
N_FS = 4
N_TP = 4


def block_levels(stream_key, extent, split, smallest, top_value):
    def one(dim, shards_of):
        steps = jax.random.uniform(jax.random.fold_in(jax.random.fold_in(stream_key, 6), dim), (shards_of,), jnp.float32, smallest / len(split), top_value / len(split))
        return jnp.repeat(jnp.exp(steps), extent[dim] // shards_of).reshape((-1,) + (1,) * (len(extent) - dim - 1))

    level = one(*split[0])
    for cut in split[1:]:
        level = level * one(*cut)
    return level


def deal_out(stream_key, own, number, rows, number_of, top, bound, lean):
    ranking = jax.random.permutation(stream_key, number_of)
    crowded, ordinary = portions_of(number_of, rows * top, bound, lean, True), portions_of(number_of, rows * top, bound, lean, False)
    places = jnp.arange(number_of)

    def named(sizes, turn):
        used = int((sizes > 0).sum())
        fixed = max(1, used // 4)
        passed = fixed + (places - fixed + turn * (used - fixed)) % max(1, number_of - fixed)
        return jnp.zeros((number_of,), jnp.int32).at[ranking[jnp.where(places < fixed, places, passed)]].set(jnp.asarray(sizes, jnp.int32))

    sizes = jnp.where(number % 4 == 0, named(crowded, number // 4), named(ordinary, number - number // 4 - 1))
    mixed = jax.random.permutation(jax.random.fold_in(own, 3), number_of)
    donor, taker = mixed[0:number_of // 2 * 2:2], mixed[1:number_of // 2 * 2:2]
    margin = jnp.minimum(sizes[donor] - 1, bound - sizes[taker]) // 2
    margin = jnp.where((donor == ranking[0]) | (taker == ranking[0]) | (sizes[taker] == 0), 0, jnp.maximum(margin, 0))
    passed = jax.random.randint(jax.random.fold_in(own, 4), (number_of // 2,), 0, 1 << 20) % (margin + 1)
    sizes = sizes.at[donor].add(-passed).at[taker].add(passed)
    members = jnp.searchsorted(jnp.cumsum(sizes), jnp.arange(rows * top), side="right").astype(jnp.int32)
    listing = members.reshape(top, rows).T
    listing = listing[jax.random.permutation(jax.random.fold_in(own, 1), rows)]
    turn = jax.random.randint(jax.random.fold_in(own, 2), (rows, 1), 0, top)
    return jnp.take_along_axis(listing, (jnp.arange(top)[None, :] + turn) % top, axis=1)


def portions_of(number_of, total, limit, slope, full):
    loads = [(1 << 20) // math.isqrt(rank ** slope) + 1 for rank in range(1, number_of + 1)]
    largest = limit if full else min(limit, max(-(-total // number_of), total * loads[0] // sum(loads)))
    least = 1 if total - largest >= number_of - 1 else 0
    counts, spare = [largest] + [least] * (number_of - 1), total - largest - least * (number_of - 1)
    while spare > 0:
        candidates = [i for i in range(1, number_of) if counts[i] < largest] or [i for i in range(1, number_of) if counts[i] < limit]
        mass, budget = sum([loads[i] for i in candidates]), spare
        for i in candidates:
            more = min(limit - counts[i], max(1, budget * loads[i] // mass), spare)
            counts[i] = counts[i] + more
            spare = spare - more
    return np.array(counts)


def centred(rng, shape, deviation, limit, cuts=(), kind=jnp.bfloat16):
    values = deviation * jax.random.normal(rng, shape, jnp.float32)
    if cuts:
        values = values * block_levels(rng, shape, cuts, -0.22, 0.18)
    return jnp.clip(values, -limit, limit).astype(kind)


def setup_inputs(seed: int = 0, part: int = 0) -> dict:
    key_list = jax.random.split(jax.random.key(seed), 8)
    part_splits = jax.random.split(jax.random.fold_in(key_list[7], part), 8)
    tokens = centred(part_splits[0], (TOKENS, D), 1.0, 6.0, ((0, 4), (1, 4)))
    route_ids_keys = jax.random.split(jax.random.fold_in(part_splits[1], 1), TOKENS // TOK_DEV)
    route_ids_turns = jax.random.permutation(jax.random.fold_in(part_splits[1], 3), TOKENS // TOK_DEV)
    route_ids = jax.vmap(lambda own, number: deal_out(jax.random.fold_in(part_splits[1], 2), own, number, TOK_DEV, EXPERTS, TOP, CAP, 1))(route_ids_keys, route_ids_turns).reshape((TOKENS, TOP))
    route_weights = jnp.clip(0.25 + 0.75 * jax.random.uniform(part_splits[2], (TOKENS, TOP), jnp.float32) ** block_levels(part_splits[2], (TOKENS, TOP), ((0, 4),), -0.2, 0.2), 0.25, 1.0)
    norm_gain = jnp.clip(1.0 + 0.18 * jax.random.normal(key_list[3], (D,), jnp.float32), 0.1, 1.9)
    gate_master = centred(key_list[4], (EXPERTS, D, F), D ** -0.5, 0.125, ((1, 4), (2, 4)), jnp.float32)
    up_master = centred(key_list[5], (EXPERTS, D, F), D ** -0.5, 0.125, ((1, 4), (2, 4)), jnp.float32)
    down_master = centred(key_list[6], (EXPERTS, D, F), F ** -0.5, 0.25, ((1, 4), (2, 4)), jnp.float32)
    return {"tokens": tokens, "route_ids": route_ids, "route_weights": route_weights, "norm_gain": norm_gain, "gate_master": gate_master, "up_master": up_master, "down_master": down_master}


norm_epsilon = 1e-06

def slot_numbers(route_ids, experts, capacity):
    flat_ids = route_ids.reshape(-1)
    onehot = (flat_ids[:, None] == jnp.arange(experts, dtype=jnp.int32)[None, :]).astype(jnp.int32)
    before = jnp.cumsum(onehot, axis=0) - onehot
    position = lax.optimization_barrier(jnp.sum(before * onehot, axis=1))
    return (flat_ids * capacity + position).astype(jnp.int32).reshape(route_ids.shape)

def reference(tokens, route_ids, route_weights, norm_gain, gate_master, up_master, down_master):
    row_gain = norm_gain[None, :, None]
    gate_serve = (gate_master * row_gain).astype(jnp.bfloat16)
    up_serve = (up_master * row_gain).astype(jnp.bfloat16)
    down_serve = down_master.astype(jnp.bfloat16)
    values = tokens.astype(jnp.float32)
    normed = (values * lax.rsqrt(lax.optimization_barrier(jnp.mean(values * values, axis=1, keepdims=True)) + norm_epsilon)).astype(jnp.bfloat16)
    blocks = normed.reshape(N_FS, TOK_DEV, D)
    expert_ids = route_ids.reshape(N_FS, TOK_DEV, TOP).astype(jnp.int32)
    slot_ids = jax.vmap(lambda ids: slot_numbers(ids, EXPERTS, CAP))(expert_ids)
    block_index = jnp.broadcast_to(jnp.arange(N_FS, dtype=jnp.int32)[:, None, None], slot_ids.shape)
    token_rows = jnp.broadcast_to(blocks[:, :, None, :], (N_FS, TOK_DEV, TOP, D))
    buffer = jnp.zeros((N_FS, EXPERTS * CAP, D), jnp.bfloat16).at[block_index, slot_ids].set(token_rows)
    by_expert = jnp.moveaxis(buffer.reshape(N_FS, EXPERTS, CAP, D), 1, 0)

    def expert_out(inputs):
        rows, gate_w, up_w, down_w = inputs
        flat_rows = rows.reshape(N_FS * CAP, D)
        gate_sum = jnp.dot(flat_rows, gate_w, preferred_element_type=jnp.float32)
        up_sum = jnp.dot(flat_rows, up_w, preferred_element_type=jnp.float32)
        hidden = (jax.nn.silu(gate_sum) * up_sum).astype(jnp.bfloat16)
        parts_hidden = hidden.astype(jnp.float32).reshape(N_FS * CAP, N_TP, F // N_TP)
        parts_down = down_w.astype(jnp.float32).reshape(D, N_TP, F // N_TP)
        partial_value = jnp.einsum('rpf,dpf->prd', parts_hidden, parts_down)
        rounded = lax.optimization_barrier(partial_value.astype(jnp.bfloat16)).astype(jnp.float32)
        return lax.optimization_barrier(jnp.sum(rounded, axis=0)).astype(jnp.bfloat16).reshape(N_FS, CAP, D)
    outputs = lax.map(expert_out, (by_expert, gate_serve, up_serve, down_serve))
    position = slot_ids - expert_ids * CAP
    picked = outputs[expert_ids, block_index, position]
    weights = route_weights.reshape(N_FS, TOK_DEV, TOP)[..., None]
    combined = lax.optimization_barrier(jnp.sum(weights * picked.astype(jnp.float32), axis=2))
    return (gate_serve, up_serve, down_serve, combined.reshape(TOKENS, D).astype(jnp.bfloat16))
```

```python
import functools
import jax
import jax.numpy as jnp
from jax import lax
from jax.experimental import pallas as pl
from jax.experimental.pallas import tpu as pltpu
from jax.sharding import PartitionSpec as P

norm_epsilon = 1e-06


def slot_numbers(route_ids, experts, capacity):
    flat_ids = route_ids.reshape(-1)
    onehot = (flat_ids[:, None] == jnp.arange(experts, dtype=jnp.int32)[None, :]).astype(jnp.int32)
    before = jnp.cumsum(onehot, axis=0) - onehot
    position = jnp.sum(before * onehot, axis=1)
    return (flat_ids * capacity + position).reshape(route_ids.shape)


def local(tokens, route_ids, route_weights, norm_gain, gate_master, up_master, down_master):
    experts = gate_master.shape[0]
    shards = lax.axis_size("fs")
    columns = lax.axis_size("tp")
    per_device = experts // shards
    tok_rows = route_ids.shape[0]
    top_count = route_ids.shape[1]
    local_width = tokens.shape[1]
    model_width = local_width * columns
    capacity = max(2, 3 * tok_rows * top_count // (2 * experts))
    row_gain = norm_gain[None, :, None]
    gate_half = (gate_master * row_gain).astype(jnp.bfloat16)
    up_half = (up_master * row_gain).astype(jnp.bfloat16)
    down_half = down_master.astype(jnp.bfloat16)
    gate_serve, up_serve, down_serve = (
        lax.all_to_all(gate_half, "fs", split_axis=0, concat_axis=1, tiled=True),
        lax.all_to_all(up_half, "fs", split_axis=0, concat_axis=1, tiled=True),
        lax.all_to_all(down_half, "fs", split_axis=0, concat_axis=1, tiled=True),
    )
    slot_ids = slot_numbers(route_ids, experts, capacity)
    slot_range = jnp.arange(experts * capacity, dtype=jnp.int32)
    selects = [
        (slot_ids[:, rank_slot, None] == slot_range[None, :]).astype(jnp.bfloat16)
        for rank_slot in range(top_count)
    ]
    placing = selects[0]
    for extra in selects[1:]:
        placing = placing + extra
    local_values = tokens.astype(jnp.float32)
    squares = lax.psum(jnp.sum(local_values * local_values, axis=1), "tp")
    inverse = lax.rsqrt(squares / model_width + norm_epsilon)[:, None]
    normed = (local_values * inverse).astype(jnp.bfloat16)
    buffer = jnp.einsum("ts,td->sd", placing, normed, preferred_element_type=jnp.float32).astype(
        jnp.bfloat16
    )
    arrived = lax.all_to_all(
        buffer.reshape(shards, per_device * capacity, local_width),
        "fs",
        split_axis=0,
        concat_axis=0,
        tiled=True,
    )
    arrived = arrived.reshape(shards, per_device, capacity, local_width)
    partial_value = lax.all_gather(arrived, "tp", axis=3, tiled=True)
    gate_sum = jnp.einsum(
        "sxcd,xdf->xscf", partial_value, gate_serve, preferred_element_type=jnp.float32
    )
    up_sum = jnp.einsum(
        "sxcd,xdf->xscf", partial_value, up_serve, preferred_element_type=jnp.float32
    )
    hidden = (jax.nn.silu(gate_sum) * up_sum).astype(jnp.bfloat16)
    products = jnp.einsum("xdf,xscf->dsxc", down_serve, hidden, preferred_element_type=jnp.float32)
    summed = lax.psum_scatter(
        products.reshape(local_width * lax.axis_size("tp"), shards * per_device * capacity).astype(
            jnp.bfloat16
        ),
        "tp",
        scatter_dimension=0,
        tiled=True,
    )
    returned = lax.all_to_all(
        summed.reshape(local_width, shards, per_device * capacity),
        "fs",
        split_axis=1,
        concat_axis=1,
        tiled=True,
    )
    returned = returned.reshape(local_width, experts * capacity)
    combined = jnp.zeros((tok_rows, local_width), jnp.float32)
    for rank_slot in range(top_count):
        picked = jnp.einsum(
            "ts,ds->td", selects[rank_slot], returned, preferred_element_type=jnp.float32
        )
        combined = combined + route_weights[:, rank_slot : rank_slot + 1] * picked
    return (gate_serve, up_serve, down_serve, combined.astype(jnp.bfloat16))


MESH = pl.DeviceIdType.MESH
bf16, f32, i32 = jnp.bfloat16, jnp.float32, jnp.int32


def remote(src, dst, send, recv, to):
    return pltpu.make_async_remote_copy(
        src_ref=src, dst_ref=dst, send_sem=send, recv_sem=recv, device_id=to, device_id_type=MESH
    )


def kernel(
    NG, NF, NT, C,
    tokens, ids, ids_t, weights, gain, gm, um, dm,
    gate_o, up_o, down_o, moe_o,
    gmv, umv, dmv, gcol, slots, xs, xg, sd, sgu, wd, wgu, wdq, hid, rs, ret,
    ld_sem, x_send, x_recv, p_sib, p_x, p_recv,
    wd_send, wd_recv, wdy_send, wdy_recv, gu_send, gu_recv, guy_send, guy_recv,
    wq_send, wq_recv, wq_own, h_sib, h_x, h_recv, r_send, r_recv, o_sem,
):
    g, f, t = lax.axis_index("grp"), lax.axis_index("fs"), lax.axis_index("tp")
    NX = NT // 2
    chip, core = t // 2, lax.rem(t, 2)
    sib = chip * 2 + (1 - core)
    H, Fl = dmv.shape[1], dmv.shape[2]
    Dl = 2 * H
    T, Dq = tokens.shape
    E = NF
    D = NT * Dq

    def fs_at(k):
        return lax.rem(f + k + NF, NF)

    def rows(s, half):
        return pl.ds(pl.multiple_of(s * Dl + half * H, H), H)

    halves = [(fs_at(k), g) for k in range(NF)] + [(f, 1 - g)]
    order = list(range(1, NF)) + [0, NF]
    loads = {}
    for m, (src, dst) in ((2, (dm, dmv)), (0, (gm, gmv)), (1, (um, umv))):
        for k in order:
            e, half = halves[k]
            cp = pltpu.make_async_copy(
                src.at[e, pl.ds(pl.multiple_of(half * H, H), H), :], dst.at[k], ld_sem.at[m, k]
            )
            cp.start()
            loads[m, k] = cp

    barrier = pltpu.get_barrier_semaphore()
    for k in range(1, NF):
        pl.semaphore_signal(barrier, inc=1, device_id={"fs": fs_at(k)}, device_id_type=MESH)
    for k in range(1, NT):
        pl.semaphore_signal(barrier, inc=1, device_id={"tp": lax.rem(t + k, NT)}, device_id_type=MESH)
    for k in range(1, NG):
        pl.semaphore_signal(barrier, inc=1, device_id={"grp": lax.rem(g + k, NG)}, device_id_type=MESH)

    member = jnp.concatenate(
        [
            jnp.max((ids_t[...] == e).astype(f32), axis=0, keepdims=True)
            for e in range(E)
        ],
        axis=0,
    )
    earlier = (
        lax.broadcasted_iota(i32, (T, T), 0) < lax.broadcasted_iota(i32, (T, T), 1)
    ).astype(bf16)
    pos = jnp.dot(member.astype(bf16), earlier, preferred_element_type=f32)
    slots[...] = jnp.where(member > 0, pos, -1.0)
    c_iota = lax.broadcasted_iota(i32, (C, T), 0).astype(f32)

    def placed(e):
        hot = (c_iota == slots[pl.ds(e, 1), :]).astype(bf16)
        return jnp.dot(hot, tokens[...], preferred_element_type=f32).astype(bf16)

    for k in range(1, NF):
        xs[k] = placed(fs_at(k))
    xg[t, f] = placed(f)
    pl.semaphore_wait(barrier, (NF - 1) + (NT - 1) + (NG - 1))

    waits = []

    def go(cp):
        cp.start()
        waits.append(cp)

    for k in (2, 1, 3, 4, 5, 6, 7):
        if k < NF:
            e = fs_at(k)
            go(remote(xs.at[k], xg.at[t, f], x_send.at[k], x_recv.at[f], {"fs": e}))

    def spread(buf, sems_sib, sems_x, sems_recv, s):
        go(remote(buf.at[t, s], buf.at[t, s], sems_sib.at[t, s], sems_recv.at[t, s], {"tp": sib}))
        for dx in range(1, NX):
            other = lax.rem(chip + dx, NX)
            go(
                remote(
                    buf.at[t, s], buf.at[t, s], sems_x.at[dx, s], sems_recv.at[t, s],
                    {"tp": other * 2 + core},
                )
            )

    def arrived(buf, sems_recv, q, s):
        remote(buf.at[q, s], buf.at[q, s], sems_recv.at[q, s], sems_recv.at[q, s], {"tp": sib}).wait_recv()

    def pass_on(buf, sems_sib, sems_recv, s):
        for dx in range(1, NX):
            q = lax.rem(chip + dx, NX) * 2 + core
            arrived(buf, sems_recv, q, s)
            go(remote(buf.at[q, s], buf.at[q, s], sems_sib.at[q, s], sems_recv.at[q, s], {"tp": sib}))

    def sib_arrived(buf, sems_recv, s):
        for dx in range(NX):
            arrived(buf, sems_recv, lax.rem(chip + dx, NX) * 2 + 1 - core, s)

    spread(xg, p_sib, p_x, p_recv, f)

    gcol[...] = jnp.transpose(jnp.broadcast_to(gain[...], (Fl, Dl)))
    for k in range(1, NF):
        e = fs_at(k)
        loads[2, k].wait()
        sd[k] = dmv[k].astype(bf16)
        go(remote(sd.at[k], wd.at[rows(f, g), :], wd_send.at[k], wd_recv.at[f], {"fs": e}))
    mine = pl.ds(pl.multiple_of(g * H, H), H)
    theirs = pl.ds(pl.multiple_of((1 - g) * H, H), H)
    for k in range(1, NF):
        e = fs_at(k)
        loads[0, k].wait()
        loads[1, k].wait()
        sgu[k, :, :Fl] = (gmv[k] * gcol[mine, :]).astype(bf16)
        sgu[k, :, Fl:] = (umv[k] * gcol[mine, :]).astype(bf16)
        go(remote(sgu.at[k], wgu.at[rows(f, g), :], gu_send.at[k], gu_recv.at[f], {"fs": e}))
    for k, half, part in ((0, g, mine), (NF, 1 - g, theirs)):
        for m in range(3):
            loads[m, k].wait()
        wd[rows(f, half), :] = dmv[k].astype(bf16)
        wgu[rows(f, half), :Fl] = (gmv[k] * gcol[part, :]).astype(bf16)
        wgu[rows(f, half), Fl:] = (umv[k] * gcol[part, :]).astype(bf16)

    near = [k for k in (1, 3, 2, 4, 5, 6, 7) if k < NF]
    for k in near:
        s = fs_at(k)
        remote(xs.at[k], xg.at[t, s], x_send.at[k], x_recv.at[s], {"fs": s}).wait_recv()
        spread(xg, p_sib, p_x, p_recv, s)
    pass_on(xg, p_sib, p_recv, f)
    for k in near:
        pass_on(xg, p_sib, p_recv, fs_at(k))

    peer = {"grp": lax.rem(g + 1, NG)}

    def to_peer(buf, send, recv, y_send, y_recv, block):
        for k in near:
            s = fs_at(k)
            remote(block.at[k], buf.at[rows(s, g), :], send.at[k], recv.at[s], {"fs": s}).wait_recv()
            go(remote(buf.at[rows(s, g), :], buf.at[rows(s, g), :], y_send.at[s], y_recv.at[s], peer))

    def from_peer(buf, y_send, y_recv):
        for k in near:
            s = fs_at(k)
            there = buf.at[rows(s, 1 - g), :]
            remote(there, there, y_send.at[s], y_recv.at[s], peer).wait_recv()

    to_peer(wd, wd_send, wd_recv, wdy_send, wdy_recv, sd)
    from_peer(wd, wdy_send, wdy_recv)

    def quarter(q):
        return wd.at[pl.ds(pl.multiple_of(q * Dq, Dq), Dq), :]

    for k in range(1, NT):
        q = lax.rem(t + k, NT)
        go(remote(quarter(q), wdq.at[t], wq_send.at[k], wq_recv.at[t], {"tp": q}))
    own_q = pltpu.make_async_copy(quarter(t), wdq.at[t], wq_own)
    own_q.start()
    outs = [pltpu.make_async_copy(wd, down_o.at[0], o_sem.at[2])]
    outs[0].start()

    for k in range(NF):
        sib_arrived(xg, p_recv, fs_at(k))
    to_peer(wgu, gu_send, gu_recv, guy_send, guy_recv, sgu)
    from_peer(wgu, guy_send, guy_recv)
    outs.append(pltpu.make_async_copy(wgu.at[:, :Fl], gate_o.at[0], o_sem.at[0]))
    outs.append(pltpu.make_async_copy(wgu.at[:, Fl:], up_o.at[0], o_sem.at[1]))
    outs[1].start()
    outs[2].start()

    far = [k for k in (2, 1, 3, 4, 5, 6, 7) if k < NF] + [0]
    for k in far:
        s = fs_at(k)
        x = jnp.concatenate([xg[q, s] for q in range(NT)], axis=1)
        xf = x.astype(f32)
        inv = lax.rsqrt(jnp.sum(xf * xf, axis=1, keepdims=True) / D + norm_epsilon)
        both = jnp.dot(x, wgu[...], preferred_element_type=f32) * inv
        gate, up = both[:, :Fl], both[:, Fl:]
        hid[t, s] = (gate / (1.0 + jnp.exp(-gate)) * up).astype(bf16)
        spread(hid, h_sib, h_x, h_recv, s)
    own_q.wait()
    for k in range(1, NT):
        q = lax.rem(t + k, NT)
        remote(wdq.at[q], wdq.at[q], wq_send.at[k], wq_recv.at[q], {"tp": q}).wait_recv()
    for k in far:
        pass_on(hid, h_sib, h_recv, fs_at(k))
    for k in far:
        s = fs_at(k)
        sib_arrived(hid, h_recv, s)
        h = jnp.concatenate([hid[q, s] for q in range(NT)], axis=1)
        w = jnp.concatenate([wdq[q] for q in range(NT)], axis=1)
        y = lax.dot_general(h, w, (((1,), (1,)), ((), ())), preferred_element_type=f32).astype(bf16)
        if k == 0:
            ret[f] = y
        else:
            rs[k] = y
            go(remote(rs.at[k], ret.at[f], r_send.at[k], r_recv.at[f], {"fs": s}))

    K = ids.shape[1]
    lane_e = lax.broadcasted_iota(i32, (T, 128), 1)
    chosen = [ids[:, k : k + 1] for k in range(K)]
    memb = sum((c == lane_e).astype(f32) for c in chosen)
    before = (
        lax.broadcasted_iota(i32, (T, T), 1) < lax.broadcasted_iota(i32, (T, T), 0)
    ).astype(bf16)
    place = jnp.dot(before, memb.astype(bf16), preferred_element_type=f32)
    c_lane = lax.broadcasted_iota(i32, (T, C), 1).astype(f32)
    total = [jnp.zeros((T, Dq), f32) for _ in range(K)]
    for k in [0] + near:
        e = fs_at(k)
        slot = jnp.sum(jnp.where(lane_e == e, place, 0.0), axis=1, keepdims=True)
        hits = [(c_lane == jnp.where(c == e, slot, -1.0)).astype(bf16) for c in chosen]
        if k:
            remote(rs.at[k], ret.at[e], r_send.at[k], r_recv.at[e], {"fs": e}).wait_recv()
        block = ret[e]
        total = [
            old + jnp.dot(hit, block, preferred_element_type=f32) for old, hit in zip(total, hits)
        ]
    out = sum(weights[:, k : k + 1] * total[k] for k in range(K))
    moe_o[...] = out.astype(bf16)
    for cp in outs:
        cp.wait()
    for cp in waits:
        cp.wait_send()


def fused(tokens, route_ids, route_weights, norm_gain, gate_master, up_master, down_master):
    NG, NF, NT = (lax.axis_size(a) for a in ("grp", "fs", "tp"))
    E, Dl, Fl = gate_master.shape
    T, Dq = tokens.shape
    capacity = max(2, 3 * T * route_ids.shape[1] // (2 * E))
    C = -(-capacity // 16) * 16
    H = Dl // 2
    D = Dl * NF
    NX = NT // 2
    dma = pltpu.SemaphoreType.DMA
    vmem, hbm = pl.BlockSpec(memory_space=pltpu.VMEM), pl.BlockSpec(memory_space=pl.ANY)
    serve = jax.ShapeDtypeStruct((1, D, Fl), bf16)
    return pl.pallas_call(
        functools.partial(kernel, NG, NF, NT, C),
        out_shape=(serve, serve, serve, jax.ShapeDtypeStruct((T, Dq), bf16)),
        in_specs=[vmem] * 5 + [hbm] * 3,
        out_specs=(hbm, hbm, hbm, vmem),
        scratch_shapes=[
            pltpu.VMEM((NF + 1, H, Fl), f32),
            pltpu.VMEM((NF + 1, H, Fl), f32),
            pltpu.VMEM((NF + 1, H, Fl), f32),
            pltpu.VMEM((Dl, Fl), f32),
            pltpu.VMEM((E, T), f32),
            pltpu.VMEM((NF, C, Dq), bf16),
            pltpu.VMEM((NT, NF, C, Dq), bf16),
            pltpu.VMEM((NF, H, Fl), bf16),
            pltpu.VMEM((NF, H, 2 * Fl), bf16),
            pltpu.VMEM((D, Fl), bf16),
            pltpu.VMEM((D, 2 * Fl), bf16),
            pltpu.VMEM((NT, Dq, Fl), bf16),
            pltpu.VMEM((NT, NF, C, Fl), bf16),
            pltpu.VMEM((NF, C, Dq), bf16),
            pltpu.VMEM((NF, C, Dq), bf16),
            dma((3, NF + 1)),
            dma((NF,)), dma((NF,)),
            dma((NT, NF)), dma((NX, NF)), dma((NT, NF)),
            dma((NF,)), dma((NF,)), dma((NF,)), dma((NF,)),
            dma((NF,)), dma((NF,)), dma((NF,)), dma((NF,)),
            dma((NT,)), dma((NT,)), dma(()),
            dma((NT, NF)), dma((NX, NF)), dma((NT, NF)),
            dma((NF,)), dma((NF,)),
            dma((3,)),
        ],
        compiler_params=pltpu.CompilerParams(
            collective_id=0, has_side_effects=True, vmem_limit_bytes=56 * 1024 * 1024
        ),
    )(
        tokens, route_ids, route_ids.T, route_weights, norm_gain[None, :],
        gate_master, up_master, down_master,
    )


def solution(mesh):
    shape = mesh.shape
    fits = shape['grp'] == 2 and shape['tp'] % 2 == 0 and shape['fs'] <= 8
    body = fused if fits else local
    placed = (
        P(("grp", "fs"), "tp"),
        P(("grp", "fs"), None),
        P(("grp", "fs"), None),
        P("fs"),
        P(None, "fs", "tp"),
        P(None, "fs", "tp"),
        P(None, "fs", "tp"),
    )
    return jax.shard_map(
        body,
        mesh=mesh,
        in_specs=placed,
        out_specs=(
            P(("grp", "fs"), None, "tp"),
            P(("grp", "fs"), None, "tp"),
            P(("grp", "fs"), None, "tp"),
            P(("grp", "fs"), "tp"),
        ),
        check_vma=False,
    )
```

```python
import functools
import jax
import jax.numpy as jnp
from jax import lax
from jax.experimental import pallas as pl
from jax.experimental.pallas import tpu as pltpu
from jax.sharding import PartitionSpec as P

norm_epsilon = 1e-06


def slot_numbers(route_ids, experts, capacity):
    flat_ids = route_ids.reshape(-1)
    onehot = (flat_ids[:, None] == jnp.arange(experts, dtype=jnp.int32)[None, :]).astype(jnp.int32)
    before = jnp.cumsum(onehot, axis=0) - onehot
    position = jnp.sum(before * onehot, axis=1)
    return (flat_ids * capacity + position).reshape(route_ids.shape)


def local(tokens, route_ids, route_weights, norm_gain, gate_master, up_master, down_master):
    experts = gate_master.shape[0]
    shards = lax.axis_size("fs")
    columns = lax.axis_size("tp")
    per_device = experts // shards
    tok_rows = route_ids.shape[0]
    top_count = route_ids.shape[1]
    local_width = tokens.shape[1]
    model_width = local_width * columns
    capacity = max(2, 3 * tok_rows * top_count // (2 * experts))
    row_gain = norm_gain[None, :, None]
    gate_half = (gate_master * row_gain).astype(jnp.bfloat16)
    up_half = (up_master * row_gain).astype(jnp.bfloat16)
    down_half = down_master.astype(jnp.bfloat16)
    gate_serve, up_serve, down_serve = (
        lax.all_to_all(gate_half, "fs", split_axis=0, concat_axis=1, tiled=True),
        lax.all_to_all(up_half, "fs", split_axis=0, concat_axis=1, tiled=True),
        lax.all_to_all(down_half, "fs", split_axis=0, concat_axis=1, tiled=True),
    )
    slot_ids = slot_numbers(route_ids, experts, capacity)
    slot_range = jnp.arange(experts * capacity, dtype=jnp.int32)
    selects = [
        (slot_ids[:, rank_slot, None] == slot_range[None, :]).astype(jnp.bfloat16)
        for rank_slot in range(top_count)
    ]
    placing = selects[0]
    for extra in selects[1:]:
        placing = placing + extra
    local_values = tokens.astype(jnp.float32)
    squares = lax.psum(jnp.sum(local_values * local_values, axis=1), "tp")
    inverse = lax.rsqrt(squares / model_width + norm_epsilon)[:, None]
    normed = (local_values * inverse).astype(jnp.bfloat16)
    buffer = jnp.einsum("ts,td->sd", placing, normed, preferred_element_type=jnp.float32).astype(
        jnp.bfloat16
    )
    arrived = lax.all_to_all(
        buffer.reshape(shards, per_device * capacity, local_width),
        "fs",
        split_axis=0,
        concat_axis=0,
        tiled=True,
    )
    arrived = arrived.reshape(shards, per_device, capacity, local_width)
    partial_value = lax.all_gather(arrived, "tp", axis=3, tiled=True)
    gate_sum = jnp.einsum(
        "sxcd,xdf->xscf", partial_value, gate_serve, preferred_element_type=jnp.float32
    )
    up_sum = jnp.einsum(
        "sxcd,xdf->xscf", partial_value, up_serve, preferred_element_type=jnp.float32
    )
    hidden = (jax.nn.silu(gate_sum) * up_sum).astype(jnp.bfloat16)
    products = jnp.einsum("xdf,xscf->dsxc", down_serve, hidden, preferred_element_type=jnp.float32)
    summed = lax.psum_scatter(
        products.reshape(local_width * lax.axis_size("tp"), shards * per_device * capacity).astype(
            jnp.bfloat16
        ),
        "tp",
        scatter_dimension=0,
        tiled=True,
    )
    returned = lax.all_to_all(
        summed.reshape(local_width, shards, per_device * capacity),
        "fs",
        split_axis=1,
        concat_axis=1,
        tiled=True,
    )
    returned = returned.reshape(local_width, experts * capacity)
    combined = jnp.zeros((tok_rows, local_width), jnp.float32)
    for rank_slot in range(top_count):
        picked = jnp.einsum(
            "ts,ds->td", selects[rank_slot], returned, preferred_element_type=jnp.float32
        )
        combined = combined + route_weights[:, rank_slot : rank_slot + 1] * picked
    return (gate_serve, up_serve, down_serve, combined.astype(jnp.bfloat16))


MESH = pl.DeviceIdType.MESH
bf16, f32, i32 = jnp.bfloat16, jnp.float32, jnp.int32


def remote(src, dst, send, recv, to):
    return pltpu.make_async_remote_copy(
        src_ref=src, dst_ref=dst, send_sem=send, recv_sem=recv, device_id=to, device_id_type=MESH
    )


def kernel(
    NF, NT, C,
    tokens, ids_t, weights_t, gain, gm, um, dm,
    gate_o, up_o, down_o, moe_o,
    gmv, umv, dmv, gcol, toks, ids_all, xg, invs, acc, comb, sd, sgu, wd, wgu, wdq, hid, rs, ret,
    ld_sem, i_send, i_recv, c_send, c_recv, p_sib, p_x, p_recv,
    wd_send, wd_recv, wdy_send, wdy_recv, gu_send, gu_recv, guy_send, guy_recv,
    wq_send, wq_recv, wq_own, h_sib, h_x, h_recv, r_send, r_recv, o_sem,
):
    g, f, t = lax.axis_index("grp"), lax.axis_index("fs"), lax.axis_index("tp")
    NX = NT // 2
    chip, core = t // 2, lax.rem(t, 2)
    sib = chip * 2 + (1 - core)
    H, Fl = dmv.shape[1], dmv.shape[2]
    Dl = 2 * H
    T, Dq = tokens.shape
    D = NT * Dq
    ring = range(1, NF)

    def fs_at(k):
        return lax.rem(f + k + NF, NF)

    def rows(s, half):
        return pl.ds(pl.multiple_of(s * Dl + half * H, H), H)

    def both(s):
        return pl.ds(pl.multiple_of(s * Dl, Dl), Dl)

    halves = [(fs_at(k), g) for k in range(NF)] + [(f, 1 - g)]
    order = list(ring) + [0, NF]
    loads = {}
    for m, src, dst in ((0, gm, gmv), (1, um, umv), (2, dm, dmv)):
        for k in order:
            e, half = halves[k]
            cp = pltpu.make_async_copy(
                src.at[e, pl.ds(pl.multiple_of(half * H, H), H), :], dst.at[k], ld_sem.at[m, k]
            )
            cp.start()
            loads[m, k] = cp

    barrier = pltpu.get_barrier_semaphore()
    for k in ring:
        pl.semaphore_signal(barrier, inc=1, device_id={"fs": fs_at(k)}, device_id_type=MESH)
    for k in range(1, NT):
        pl.semaphore_signal(barrier, inc=1, device_id={"tp": lax.rem(t + k, NT)}, device_id_type=MESH)
    peer = {"grp": 1 - g}
    pl.semaphore_signal(barrier, inc=1, device_id=peer, device_id_type=MESH)

    earlier = (
        lax.broadcasted_iota(i32, (T, T), 0) < lax.broadcasted_iota(i32, (T, T), 1)
    ).astype(bf16)
    c_iota = lax.broadcasted_iota(i32, (C, T), 0).astype(f32)

    def slot_row(ids, e):
        member = jnp.max((ids == e).astype(f32), axis=0, keepdims=True)
        pos = jnp.dot(
            jnp.broadcast_to(member, (8, T)).astype(bf16), earlier, preferred_element_type=f32
        )
        return jnp.where(member > 0, pos[:1], -1.0)

    def place(s, ids, block):
        hot = (c_iota == slot_row(ids, f)).astype(bf16)
        xg[t, s] = jnp.dot(hot, block[...], preferred_element_type=f32).astype(bf16)

    pl.semaphore_wait(barrier, (NF - 1) + (NT - 1) + 1)

    waits = []

    def go(cp):
        cp.start()
        waits.append(cp)

    for k in ring:
        go(remote(ids_t, ids_all.at[f], i_send.at[k], i_recv.at[f], {"fs": fs_at(k)}))

    def hop_right(src, b):
        return remote(src, toks.at[b], c_send.at[0, b], c_recv.at[b], {"fs": f + 1})

    def hop_left(src, b):
        return remote(src, toks.at[b], c_send.at[1, b], c_recv.at[b], {"fs": f - 1})

    @pl.when(f < NF - 1)
    def _():
        hop_right(tokens, f).start()

    @pl.when(f > 0)
    def _():
        hop_left(tokens, f).start()

    def spread(buf, sems_sib, sems_x, sems_recv, s):
        for dx in range(1, NX):
            other = lax.rem(chip + dx, NX)
            remote(
                buf.at[t, s], buf.at[t, s], sems_x.at[dx, s], sems_recv.at[t, s],
                {"tp": other * 2 + core},
            ).start()
        remote(buf.at[t, s], buf.at[t, s], sems_sib.at[t, s], sems_recv.at[t, s], {"tp": sib}).start()

    def arrived(buf, sems_recv, q, s):
        remote(buf.at[q, s], buf.at[q, s], sems_recv.at[q, s], sems_recv.at[q, s], {"tp": sib}).wait_recv()

    def pass_on(buf, sems_sib, sems_recv, s):
        for dx in range(1, NX):
            q = lax.rem(chip + dx, NX) * 2 + core
            arrived(buf, sems_recv, q, s)
            remote(buf.at[q, s], buf.at[q, s], sems_sib.at[q, s], sems_recv.at[q, s], {"tp": sib}).start()

    def sib_arrived(buf, sems_recv, s):
        for dx in range(NX):
            arrived(buf, sems_recv, lax.rem(chip + dx, NX) * 2 + 1 - core, s)

    def spread_sent(buf, sems_sib, sems_x, s):
        for dx in range(1, NX):
            remote(buf.at[t, s], buf.at[t, s], sems_x.at[dx, s], sems_x.at[dx, s], {"tp": sib}).wait_send()
        for dx in range(NX):
            q = lax.rem(chip + dx, NX) * 2 + core
            remote(buf.at[q, s], buf.at[q, s], sems_sib.at[q, s], sems_sib.at[q, s], {"tp": sib}).wait_send()

    place(f, ids_t[...], tokens)
    spread(xg, p_sib, p_x, p_recv, f)

    gcol[...] = jnp.transpose(jnp.broadcast_to(gain[...], (Fl, Dl)))
    mine = pl.ds(pl.multiple_of(g * H, H), H)
    theirs = pl.ds(pl.multiple_of((1 - g) * H, H), H)
    for k in ring:
        loads[0, k].wait()
        loads[1, k].wait()
        sgu[k, :, :Fl] = (gmv[k] * gcol[mine, :]).astype(bf16)
        sgu[k, :, Fl:] = (umv[k] * gcol[mine, :]).astype(bf16)
    for k in ring:
        loads[2, k].wait()
        sd[k] = dmv[k].astype(bf16)

    def gu_copy(k, e):
        return remote(sgu.at[k], wgu.at[rows(f, g), :], gu_send.at[k], gu_recv.at[f], {"fs": e})

    def wd_copy(k, e):
        return remote(sd.at[k], wd.at[rows(f, g), :], wd_send.at[k], wd_recv.at[f], {"fs": e})

    def send_weights(at, way):
        reach = NF - 1 - at if way > 0 else at
        for make in (gu_copy, wd_copy):
            for dist in range(reach, 0, -1):
                make(way * dist % NF, at + way * dist).start()

    def weights_after(d):
        if d < NF - 1:
            @pl.when(f == d)
            def _():
                send_weights(d, 1)

            @pl.when(f == NF - 1 - d)
            def _():
                send_weights(NF - 1 - d, -1)

    weights_after(0)
    for k, half, part in ((0, g, mine), (NF, 1 - g, theirs)):
        for m in range(3):
            loads[m, k].wait()
        wd[rows(f, half), :] = dmv[k].astype(bf16)
        wgu[rows(f, half), :Fl] = (gmv[k] * gcol[part, :]).astype(bf16)
        wgu[rows(f, half), Fl:] = (umv[k] * gcol[part, :]).astype(bf16)

    for k in ring:
        s = fs_at(k)
        remote(ids_t, ids_all.at[s], i_recv.at[s], i_recv.at[s], {"fs": s}).wait_recv()

    def take(b):
        place(b, ids_all[b], toks.at[b])
        spread(xg, p_sib, p_x, p_recv, b)

    for d in ring:
        @pl.when(f >= d)
        def _():
            hop_right(tokens, f - d).wait_recv()

            @pl.when(f < NF - 1)
            def _():
                hop_right(toks.at[f - d], f - d).start()

        @pl.when(f + d < NF)
        def _():
            hop_left(tokens, f + d).wait_recv()

            @pl.when(f > 0)
            def _():
                hop_left(toks.at[f + d], f + d).start()

        weights_after(d)

        @pl.when(f >= d)
        def _():
            take(f - d)

        @pl.when(f + d < NF)
        def _():
            take(f + d)

        if d == 1:
            pass_on(xg, p_sib, p_recv, f)
        else:
            @pl.when(f >= d - 1)
            def _():
                pass_on(xg, p_sib, p_recv, f - d + 1)

            @pl.when(f + d - 1 < NF)
            def _():
                pass_on(xg, p_sib, p_recv, f + d - 1)

    near = [k for k in (1, 3, 2, 4, 5, 6, 7) if k < NF]

    def to_peer(buf, make, y_send, y_recv, recv, k):
        s = fs_at(k)
        here = buf.at[rows(s, g), :]
        remote(here, here, recv.at[s], recv.at[s], {"fs": s}).wait_recv()
        remote(here, here, y_send.at[s], y_recv.at[s], peer).start()

    def from_peer(buf, y_recv, k):
        s = fs_at(k)
        there = buf.at[rows(s, 1 - g), :]
        remote(there, there, y_recv.at[s], y_recv.at[s], peer).wait_recv()

    to_peer(wgu, gu_copy, guy_send, guy_recv, gu_recv, near[0])
    for d in (NF - 1,):
        @pl.when(f >= d)
        def _():
            pass_on(xg, p_sib, p_recv, f - d)

        @pl.when(f + d < NF)
        def _():
            pass_on(xg, p_sib, p_recv, f + d)
    for k in near[1:]:
        to_peer(wgu, gu_copy, guy_send, guy_recv, gu_recv, k)

    for e in range(NF):
        w_row = jnp.sum(jnp.where(ids_t[...] == e, weights_t[...], 0.0), axis=0, keepdims=True)
        w_at = jnp.where(c_iota == slot_row(ids_t[...], e), w_row, 0.0)
        high = w_at.astype(bf16)
        comb[e, :C] = high
        comb[e, C:] = (w_at - high.astype(f32)).astype(bf16)

    for k in range(NF):
        s = fs_at(k)
        sib_arrived(xg, p_recv, s)
        sq = jnp.zeros((C, 1), f32)
        for q in range(NT):
            xf = xg[q, s].astype(f32)
            sq = sq + jnp.sum(xf * xf, axis=1, keepdims=True)
        invs[s] = jnp.broadcast_to(lax.rsqrt(sq / D + norm_epsilon), (C, Fl))

    def partial_sums(s):
        x = xg[s].reshape(NF * C, Dq)
        return jnp.dot(x, wgu[both(s), :], preferred_element_type=f32)

    acc[...] = partial_sums(f)
    for k in near:
        from_peer(wgu, guy_recv, k)
        acc[...] += partial_sums(fs_at(k))
        to_peer(wd, wd_copy, wdy_send, wdy_recv, wd_recv, k)
    outs = [
        pltpu.make_async_copy(wgu.at[:, :Fl], gate_o.at[0], o_sem.at[0]),
        pltpu.make_async_copy(wgu.at[:, Fl:], up_o.at[0], o_sem.at[1]),
        pltpu.make_async_copy(wd, down_o.at[0], o_sem.at[2]),
    ]
    outs[0].start()
    outs[1].start()

    far = [k for k in (2, 1, 3, 4, 5, 6, 7) if k < NF] + [0]
    for k in far:
        s = fs_at(k)
        sums = acc[pl.ds(pl.multiple_of(s * C, 16), C), :]
        gate, up = sums[:, :Fl] * invs[s], sums[:, Fl:] * invs[s]
        hid[t, s] = (gate / (1.0 + jnp.exp(-gate)) * up).astype(bf16)
        spread(hid, h_sib, h_x, h_recv, s)

    def turned(s):
        return remote(wd.at[both(s), :], wdq.at[t], wq_send.at[s], wq_recv.at[t], {"tp": s})

    own_q = pltpu.make_async_copy(wd.at[both(t), :], wdq.at[t], wq_own)
    for k in [0] + near:
        s = fs_at(k)
        if k:
            from_peer(wd, wdy_recv, k)

        @pl.when(s != t)
        def _():
            turned(s).start()

        @pl.when(s == t)
        def _():
            own_q.start()
    outs[2].start()
    for k in far:
        pass_on(hid, h_sib, h_recv, fs_at(k))
    own_q.wait()
    for k in range(1, NT):
        q = lax.rem(t + k, NT)
        remote(wdq.at[q], wdq.at[q], wq_recv.at[q], wq_recv.at[q], {"tp": q}).wait_recv()
    for k in far:
        s = fs_at(k)
        sib_arrived(hid, h_recv, s)
        h = jnp.concatenate([hid[q, s] for q in range(NT)], axis=1)
        w = jnp.concatenate([wdq[q] for q in range(NT)], axis=1)
        y = lax.dot_general(h, w, (((1,), (1,)), ((), ())), preferred_element_type=f32).astype(bf16)
        if k == 0:
            ret[f] = y
        else:
            rs[k] = y
            go(remote(rs.at[k], ret.at[f], r_send.at[k], r_recv.at[f], {"fs": s}))

    total = jnp.zeros((T, Dq), f32)
    for k in [0] + near:
        e = fs_at(k)
        if k:
            remote(rs.at[k], ret.at[e], r_send.at[k], r_recv.at[e], {"fs": e}).wait_recv()
        block = jnp.concatenate([ret[e], ret[e]], axis=0)
        total = total + lax.dot_general(
            comb[e], block, (((0,), (0,)), ((), ())), preferred_element_type=f32
        )
    moe_o[...] = total.astype(bf16)

    for cp in outs:
        cp.wait()
    for cp in waits:
        cp.wait_send()
    for k in ring:
        s = fs_at(k)
        gu_copy(k, s).wait_send()
        wd_copy(k, s).wait_send()
        for buf, y_send in ((wgu, guy_send), (wd, wdy_send)):
            here = buf.at[rows(s, g), :]
            remote(here, here, y_send.at[s], y_send.at[s], peer).wait_send()
    for s in range(NF):
        @pl.when(s != t)
        def _():
            turned(s).wait_send()

        spread_sent(xg, p_sib, p_x, s)
        spread_sent(hid, h_sib, h_x, s)

        @pl.when((s <= f) & (f < NF - 1))
        def _():
            hop_right(tokens, s).wait_send()

        @pl.when((s >= f) & (f > 0))
        def _():
            hop_left(tokens, s).wait_send()


def fused(tokens, route_ids, route_weights, norm_gain, gate_master, up_master, down_master):
    NF, NT = lax.axis_size("fs"), lax.axis_size("tp")
    E, Dl, Fl = gate_master.shape
    T, Dq = tokens.shape
    K = route_ids.shape[1]
    capacity = max(2, 3 * T * K // (2 * E))
    C = -(-capacity // 16) * 16
    H = Dl // 2
    D = Dl * NF
    NX = NT // 2
    dma = pltpu.SemaphoreType.DMA
    vmem, hbm = pl.BlockSpec(memory_space=pltpu.VMEM), pl.BlockSpec(memory_space=pl.ANY)
    serve = jax.ShapeDtypeStruct((1, D, Fl), bf16)
    return pl.pallas_call(
        functools.partial(kernel, NF, NT, C),
        out_shape=(serve, serve, serve, jax.ShapeDtypeStruct((T, Dq), bf16)),
        in_specs=[vmem] * 4 + [hbm] * 3,
        out_specs=(hbm, hbm, hbm, vmem),
        scratch_shapes=[
            pltpu.VMEM((NF + 1, H, Fl), f32),
            pltpu.VMEM((NF + 1, H, Fl), f32),
            pltpu.VMEM((NF + 1, H, Fl), f32),
            pltpu.VMEM((Dl, Fl), f32),
            pltpu.VMEM((NF, T, Dq), bf16),
            pltpu.VMEM((NF, K, T), i32),
            pltpu.VMEM((NT, NF, C, Dq), bf16),
            pltpu.VMEM((NF, C, Fl), f32),
            pltpu.VMEM((NF * C, 2 * Fl), f32),
            pltpu.VMEM((NF, 2 * C, T), bf16),
            pltpu.VMEM((NF, H, Fl), bf16),
            pltpu.VMEM((NF, H, 2 * Fl), bf16),
            pltpu.VMEM((D, Fl), bf16),
            pltpu.VMEM((D, 2 * Fl), bf16),
            pltpu.VMEM((NT, Dq, Fl), bf16),
            pltpu.VMEM((NT, NF, C, Fl), bf16),
            pltpu.VMEM((NF, C, Dq), bf16),
            pltpu.VMEM((NF, C, Dq), bf16),
            dma((3, NF + 1)),
            dma((NF,)), dma((NF,)),
            dma((2, NF)), dma((NF,)),
            dma((NT, NF)), dma((NX, NF)), dma((NT, NF)),
            dma((NF,)), dma((NF,)), dma((NF,)), dma((NF,)),
            dma((NF,)), dma((NF,)), dma((NF,)), dma((NF,)),
            dma((NT,)), dma((NT,)), dma(()),
            dma((NT, NF)), dma((NX, NF)), dma((NT, NF)),
            dma((NF,)), dma((NF,)),
            dma((3,)),
        ],
        compiler_params=pltpu.CompilerParams(
            collective_id=0, has_side_effects=True, vmem_limit_bytes=56 * 1024 * 1024
        ),
    )(
        tokens, route_ids.T, route_weights.T, norm_gain[None, :],
        gate_master, up_master, down_master,
    )


def solution(mesh):
    shape = mesh.shape
    fits = shape['grp'] == 2 and shape['tp'] % 2 == 0 and shape['fs'] == shape['tp'] <= 8
    body = fused if fits else local
    placed = (
        P(("grp", "fs"), "tp"),
        P(("grp", "fs"), None),
        P(("grp", "fs"), None),
        P("fs"),
        P(None, "fs", "tp"),
        P(None, "fs", "tp"),
        P(None, "fs", "tp"),
    )
    return jax.shard_map(
        body,
        mesh=mesh,
        in_specs=placed,
        out_specs=(
            P(("grp", "fs"), None, "tp"),
            P(("grp", "fs"), None, "tp"),
            P(("grp", "fs"), None, "tp"),
            P(("grp", "fs"), "tp"),
        ),
        check_vma=False,
    )
```

```python
import functools
import jax
import jax.numpy as jnp
from jax import lax
from jax.experimental import pallas as pl
from jax.experimental.pallas import tpu as pltpu
from jax.sharding import PartitionSpec as P

norm_epsilon = 1e-06


def slot_numbers(route_ids, experts, capacity):
    flat_ids = route_ids.reshape(-1)
    onehot = (flat_ids[:, None] == jnp.arange(experts, dtype=jnp.int32)[None, :]).astype(jnp.int32)
    before = jnp.cumsum(onehot, axis=0) - onehot
    position = jnp.sum(before * onehot, axis=1)
    return (flat_ids * capacity + position).reshape(route_ids.shape)


def local(tokens, route_ids, route_weights, norm_gain, gate_master, up_master, down_master):
    experts = gate_master.shape[0]
    shards = lax.axis_size("fs")
    columns = lax.axis_size("tp")
    per_device = experts // shards
    tok_rows = route_ids.shape[0]
    top_count = route_ids.shape[1]
    local_width = tokens.shape[1]
    model_width = local_width * columns
    capacity = max(2, 3 * tok_rows * top_count // (2 * experts))
    row_gain = norm_gain[None, :, None]
    gate_half = (gate_master * row_gain).astype(jnp.bfloat16)
    up_half = (up_master * row_gain).astype(jnp.bfloat16)
    down_half = down_master.astype(jnp.bfloat16)
    gate_serve, up_serve, down_serve = (
        lax.all_to_all(gate_half, "fs", split_axis=0, concat_axis=1, tiled=True),
        lax.all_to_all(up_half, "fs", split_axis=0, concat_axis=1, tiled=True),
        lax.all_to_all(down_half, "fs", split_axis=0, concat_axis=1, tiled=True),
    )
    slot_ids = slot_numbers(route_ids, experts, capacity)
    slot_range = jnp.arange(experts * capacity, dtype=jnp.int32)
    selects = [
        (slot_ids[:, rank_slot, None] == slot_range[None, :]).astype(jnp.bfloat16)
        for rank_slot in range(top_count)
    ]
    placing = selects[0]
    for extra in selects[1:]:
        placing = placing + extra
    local_values = tokens.astype(jnp.float32)
    squares = lax.psum(jnp.sum(local_values * local_values, axis=1), "tp")
    inverse = lax.rsqrt(squares / model_width + norm_epsilon)[:, None]
    normed = (local_values * inverse).astype(jnp.bfloat16)
    buffer = jnp.einsum("ts,td->sd", placing, normed, preferred_element_type=jnp.float32).astype(
        jnp.bfloat16
    )
    arrived = lax.all_to_all(
        buffer.reshape(shards, per_device * capacity, local_width),
        "fs",
        split_axis=0,
        concat_axis=0,
        tiled=True,
    )
    arrived = arrived.reshape(shards, per_device, capacity, local_width)
    partial_value = lax.all_gather(arrived, "tp", axis=3, tiled=True)
    gate_sum = jnp.einsum(
        "sxcd,xdf->xscf", partial_value, gate_serve, preferred_element_type=jnp.float32
    )
    up_sum = jnp.einsum(
        "sxcd,xdf->xscf", partial_value, up_serve, preferred_element_type=jnp.float32
    )
    hidden = (jax.nn.silu(gate_sum) * up_sum).astype(jnp.bfloat16)
    products = jnp.einsum("xdf,xscf->dsxc", down_serve, hidden, preferred_element_type=jnp.float32)
    summed = lax.psum_scatter(
        products.reshape(local_width * lax.axis_size("tp"), shards * per_device * capacity).astype(
            jnp.bfloat16
        ),
        "tp",
        scatter_dimension=0,
        tiled=True,
    )
    returned = lax.all_to_all(
        summed.reshape(local_width, shards, per_device * capacity),
        "fs",
        split_axis=1,
        concat_axis=1,
        tiled=True,
    )
    returned = returned.reshape(local_width, experts * capacity)
    combined = jnp.zeros((tok_rows, local_width), jnp.float32)
    for rank_slot in range(top_count):
        picked = jnp.einsum(
            "ts,ds->td", selects[rank_slot], returned, preferred_element_type=jnp.float32
        )
        combined = combined + route_weights[:, rank_slot : rank_slot + 1] * picked
    return (gate_serve, up_serve, down_serve, combined.astype(jnp.bfloat16))


MESH = pl.DeviceIdType.MESH
bf16, f32, i32 = jnp.bfloat16, jnp.float32, jnp.int32


def remote(src, dst, send, recv, to):
    return pltpu.make_async_remote_copy(
        src_ref=src, dst_ref=dst, send_sem=send, recv_sem=recv, device_id=to, device_id_type=MESH
    )


def kernel(
    NF, NT, C,
    tokens, ids_t, weights_t, gain, gm, um, dm,
    gate_o, up_o, down_o, moe_o,
    gmv, umv, dmv, gcol, toks, ids_all, xg, invs, acc, comb, sd, sgu, wd, wgu, wdq, hid, rs, ret,
    ld_sem, i_send, i_recv, c_send, c_recv, p_sib, p_x, p_recv,
    wd_send, wd_recv, wdy_send, wdy_recv, gu_send, gu_recv, guy_send, guy_recv,
    wq_send, wq_recv, wq_own, h_sib, h_x, h_recv, r_send, r_recv, o_sem,
):
    g, f, t = lax.axis_index("grp"), lax.axis_index("fs"), lax.axis_index("tp")
    NX = NT // 2
    chip, core = t // 2, lax.rem(t, 2)
    sib = chip * 2 + (1 - core)
    H, Fl = dmv.shape[1], dmv.shape[2]
    Dl = 2 * H
    T, Dq = tokens.shape
    D = NT * Dq
    ring = range(1, NF)

    def fs_at(k):
        return lax.rem(f + k + NF, NF)

    def rows(s, half):
        return pl.ds(pl.multiple_of(s * Dl + half * H, H), H)

    def both(s):
        return pl.ds(pl.multiple_of(s * Dl, Dl), Dl)

    halves = [(fs_at(k), g) for k in range(NF)] + [(f, 1 - g)]
    order = list(ring) + [0, NF]
    loads = {}
    for m, src, dst in ((0, gm, gmv), (1, um, umv), (2, dm, dmv)):
        for k in order:
            e, half = halves[k]
            cp = pltpu.make_async_copy(
                src.at[e, pl.ds(pl.multiple_of(half * H, H), H), :], dst.at[k], ld_sem.at[m, k]
            )
            cp.start()
            loads[m, k] = cp

    barrier = pltpu.get_barrier_semaphore()
    for k in ring:
        pl.semaphore_signal(barrier, inc=1, device_id={"fs": fs_at(k)}, device_id_type=MESH)
    for k in range(1, NT):
        pl.semaphore_signal(barrier, inc=1, device_id={"tp": lax.rem(t + k, NT)}, device_id_type=MESH)
    peer = {"grp": 1 - g}
    pl.semaphore_signal(barrier, inc=1, device_id=peer, device_id_type=MESH)

    earlier = (
        lax.broadcasted_iota(i32, (T, T), 0) < lax.broadcasted_iota(i32, (T, T), 1)
    ).astype(bf16)
    c_iota = lax.broadcasted_iota(i32, (C, T), 0).astype(f32)

    def slot_row(ids, e):
        member = jnp.max((ids == e).astype(f32), axis=0, keepdims=True)
        pos = jnp.dot(
            jnp.broadcast_to(member, (8, T)).astype(bf16), earlier, preferred_element_type=f32
        )
        return jnp.where(member > 0, pos[:1], -1.0)

    def place(s, ids, block):
        hot = (c_iota == slot_row(ids, f)).astype(bf16)
        xg[t, s] = jnp.dot(hot, block[...], preferred_element_type=f32).astype(bf16)

    pl.semaphore_wait(barrier, (NF - 1) + (NT - 1) + 1)

    waits = []

    def go(cp):
        cp.start()
        waits.append(cp)

    for k in ring:
        go(remote(ids_t, ids_all.at[f], i_send.at[k], i_recv.at[f], {"fs": fs_at(k)}))

    def hop_right(src, b):
        return remote(src, toks.at[b], c_send.at[0, b], c_recv.at[b], {"fs": f + 1})

    def hop_left(src, b):
        return remote(src, toks.at[b], c_send.at[1, b], c_recv.at[b], {"fs": f - 1})

    @pl.when(f < NF - 1)
    def _():
        hop_right(tokens, f).start()

    @pl.when(f > 0)
    def _():
        hop_left(tokens, f).start()

    def spread(buf, sems_sib, sems_x, sems_recv, s):
        for dx in range(1, NX):
            other = lax.rem(chip + dx, NX)
            remote(
                buf.at[t, s], buf.at[t, s], sems_x.at[dx, s], sems_recv.at[t, s],
                {"tp": other * 2 + core},
            ).start()
        remote(buf.at[t, s], buf.at[t, s], sems_sib.at[t, s], sems_recv.at[t, s], {"tp": sib}).start()

    def arrived(buf, sems_recv, q, s):
        remote(buf.at[q, s], buf.at[q, s], sems_recv.at[q, s], sems_recv.at[q, s], {"tp": sib}).wait_recv()

    def pass_on(buf, sems_sib, sems_recv, s):
        for dx in range(1, NX):
            q = lax.rem(chip + dx, NX) * 2 + core
            arrived(buf, sems_recv, q, s)
            remote(buf.at[q, s], buf.at[q, s], sems_sib.at[q, s], sems_recv.at[q, s], {"tp": sib}).start()

    def sib_arrived(buf, sems_recv, s):
        for dx in range(NX):
            arrived(buf, sems_recv, lax.rem(chip + dx, NX) * 2 + 1 - core, s)

    def spread_sent(buf, sems_sib, sems_x, s):
        for dx in range(1, NX):
            remote(buf.at[t, s], buf.at[t, s], sems_x.at[dx, s], sems_x.at[dx, s], {"tp": sib}).wait_send()
        for dx in range(NX):
            q = lax.rem(chip + dx, NX) * 2 + core
            remote(buf.at[q, s], buf.at[q, s], sems_sib.at[q, s], sems_sib.at[q, s], {"tp": sib}).wait_send()

    place(f, ids_t[...], tokens)
    spread(xg, p_sib, p_x, p_recv, f)

    gcol[...] = jnp.transpose(jnp.broadcast_to(gain[...], (Fl, Dl)))
    mine = pl.ds(pl.multiple_of(g * H, H), H)
    theirs = pl.ds(pl.multiple_of((1 - g) * H, H), H)
    for k in ring:
        loads[0, k].wait()
        loads[1, k].wait()
        sgu[k, :, :Fl] = (gmv[k] * gcol[mine, :]).astype(bf16)
        sgu[k, :, Fl:] = (umv[k] * gcol[mine, :]).astype(bf16)
    for k in ring:
        loads[2, k].wait()
        sd[k] = dmv[k].astype(bf16)

    def gu_copy(k, e):
        return remote(sgu.at[k], wgu.at[rows(f, g), :], gu_send.at[k], gu_recv.at[f], {"fs": e})

    def wd_copy(k, e):
        return remote(sd.at[k], wd.at[rows(f, g), :], wd_send.at[k], wd_recv.at[f], {"fs": e})

    def send_weights(at, way):
        reach = NF - 1 - at if way > 0 else at
        jobs = [(gu_copy, dist) for dist in range(1, reach + 1)]
        jobs += [(wd_copy, dist) for dist in range(1, reach + 1)]
        if reach == NF - 1:
            jobs.remove((wd_copy, 1))
            jobs.insert(1, (wd_copy, 1))
        for make, dist in jobs:
            make(way * dist % NF, at + way * dist).start()

    def weights_after(d):
        if d < NF - 1:
            @pl.when(f == d)
            def _():
                send_weights(d, 1)

            @pl.when(f == NF - 1 - d)
            def _():
                send_weights(NF - 1 - d, -1)

    weights_after(0)
    for k, half, part in ((0, g, mine), (NF, 1 - g, theirs)):
        for m in range(3):
            loads[m, k].wait()
        wd[rows(f, half), :] = dmv[k].astype(bf16)
        wgu[rows(f, half), :Fl] = (gmv[k] * gcol[part, :]).astype(bf16)
        wgu[rows(f, half), Fl:] = (umv[k] * gcol[part, :]).astype(bf16)

    for k in ring:
        s = fs_at(k)
        remote(ids_t, ids_all.at[s], i_recv.at[s], i_recv.at[s], {"fs": s}).wait_recv()

    def take(b):
        place(b, ids_all[b], toks.at[b])
        spread(xg, p_sib, p_x, p_recv, b)

    for d in ring:
        @pl.when(f >= d)
        def _():
            hop_right(tokens, f - d).wait_recv()

            @pl.when(f < NF - 1)
            def _():
                hop_right(toks.at[f - d], f - d).start()

        @pl.when(f + d < NF)
        def _():
            hop_left(tokens, f + d).wait_recv()

            @pl.when(f > 0)
            def _():
                hop_left(toks.at[f + d], f + d).start()

        weights_after(d)

        @pl.when(f >= d)
        def _():
            take(f - d)

        @pl.when(f + d < NF)
        def _():
            take(f + d)

        if d == 1:
            pass_on(xg, p_sib, p_recv, f)
        else:
            @pl.when(f >= d - 1)
            def _():
                pass_on(xg, p_sib, p_recv, f - d + 1)

            @pl.when(f + d - 1 < NF)
            def _():
                pass_on(xg, p_sib, p_recv, f + d - 1)

    by_distance = [sorted((s for s in range(NF) if s != a), key=lambda s: abs(s - a)) for a in range(NF)]

    def pick(column):
        out = jnp.int32(column[0])
        for a in range(1, NF):
            out = jnp.where(f == a, jnp.int32(column[a]), out)
        return out

    near = [pick([by_distance[a][i] for a in range(NF)]) for i in range(NF - 1)]

    def to_peer(buf, y_send, y_recv, recv, s):
        here = buf.at[rows(s, g), :]
        remote(here, here, recv.at[s], recv.at[s], {"fs": s}).wait_recv()
        remote(here, here, y_send.at[s], y_recv.at[s], peer).start()

    def from_peer(buf, y_recv, s):
        there = buf.at[rows(s, 1 - g), :]
        remote(there, there, y_recv.at[s], y_recv.at[s], peer).wait_recv()

    to_peer(wgu, guy_send, guy_recv, gu_recv, near[0])
    for d in (NF - 1,):
        @pl.when(f >= d)
        def _():
            pass_on(xg, p_sib, p_recv, f - d)

        @pl.when(f + d < NF)
        def _():
            pass_on(xg, p_sib, p_recv, f + d)
    for s in near[1:]:
        to_peer(wgu, guy_send, guy_recv, gu_recv, s)

    for e in range(NF):
        w_row = jnp.sum(jnp.where(ids_t[...] == e, weights_t[...], 0.0), axis=0, keepdims=True)
        w_at = jnp.where(c_iota == slot_row(ids_t[...], e), w_row, 0.0)
        high = w_at.astype(bf16)
        comb[e, 0] = high
        comb[e, 1] = (w_at - high.astype(f32)).astype(bf16)

    for k in range(NF):
        s = fs_at(k)
        sib_arrived(xg, p_recv, s)
        sq = jnp.zeros((C, 1), f32)
        for q in range(NT):
            xf = xg[q, s].astype(f32)
            sq = sq + jnp.sum(xf * xf, axis=1, keepdims=True)
        invs[s] = jnp.broadcast_to(lax.rsqrt(sq / D + norm_epsilon), (C, Fl))

    def partial_sums(q, first):
        w = wgu[both(q), :]
        for s in range(NF):
            part = jnp.dot(xg[q, s], w, preferred_element_type=f32)
            acc[s] = part if first else acc[s] + part

    def turned(s, half):
        part = pl.ds(pl.multiple_of(half * H, H), H)
        return remote(
            wd.at[rows(s, half), :], wdq.at[t, part, :], wq_send.at[s, half], wq_recv.at[t, half], {"tp": s}
        )

    own_q = pltpu.make_async_copy(wd.at[both(t), :], wdq.at[t], wq_own)

    def turn(s, half):
        @pl.when(s != t)
        def _():
            turned(s, half).start()

    turn(f, 0)
    turn(f, 1)
    partial_sums(f, True)
    for s in near:
        from_peer(wgu, guy_recv, s)
        partial_sums(s, False)
        to_peer(wd, wdy_send, wdy_recv, wd_recv, s)
        turn(s, g)
    outs = [
        pltpu.make_async_copy(wgu.at[:, :Fl], gate_o.at[0], o_sem.at[0]),
        pltpu.make_async_copy(wgu.at[:, Fl:], up_o.at[0], o_sem.at[1]),
        pltpu.make_async_copy(wd, down_o.at[0], o_sem.at[2]),
    ]
    outs[0].start()
    outs[1].start()

    far = near[::-1] + [f]
    for s in far:
        sums = acc[s]
        gate, up = sums[:, :Fl] * invs[s], sums[:, Fl:] * invs[s]
        hid[t, s] = (gate / (1.0 + jnp.exp(-gate)) * up).astype(bf16)
        spread(hid, h_sib, h_x, h_recv, s)

    for s in near:
        from_peer(wd, wdy_recv, s)
        turn(s, 1 - g)
    own_q.start()
    outs[2].start()
    for s in far:
        pass_on(hid, h_sib, h_recv, s)
    own_q.wait()
    for k in range(1, NT):
        q = lax.rem(t + k, NT)
        for half in range(2):
            part = wdq.at[q, half * H : (half + 1) * H, :]
            remote(part, part, wq_recv.at[q, half], wq_recv.at[q, half], {"tp": q}).wait_recv()
    for i, s in enumerate(far):
        sib_arrived(hid, h_recv, s)
        h = jnp.concatenate([hid[q, s] for q in range(NT)], axis=1)
        w = jnp.concatenate([wdq[q] for q in range(NT)], axis=1)
        y = lax.dot_general(h, w, (((1,), (1,)), ((), ())), preferred_element_type=f32).astype(bf16)
        if i == NF - 1:
            ret[f] = y
        else:
            rs[s] = y
            go(remote(rs.at[s], ret.at[f], r_send.at[s], r_recv.at[f], {"fs": s}))

    total = jnp.zeros((T, Dq), f32)
    for i, e in enumerate([f] + near):
        if i:
            remote(rs.at[e], ret.at[e], r_recv.at[e], r_recv.at[e], {"fs": e}).wait_recv()
        for term in range(2):
            total = total + lax.dot_general(
                comb[e, term], ret[e], (((0,), (0,)), ((), ())), preferred_element_type=f32
            )
    moe_o[...] = total.astype(bf16)

    for cp in outs:
        cp.wait()
    for cp in waits:
        cp.wait_send()
    for k in ring:
        s = fs_at(k)
        gu_copy(k, s).wait_send()
        wd_copy(k, s).wait_send()
        for buf, y_send in ((wgu, guy_send), (wd, wdy_send)):
            here = buf.at[rows(s, g), :]
            remote(here, here, y_send.at[s], y_send.at[s], peer).wait_send()
    for s in range(NF):
        @pl.when(s != t)
        def _():
            turned(s, 0).wait_send()
            turned(s, 1).wait_send()

        spread_sent(xg, p_sib, p_x, s)
        spread_sent(hid, h_sib, h_x, s)

        @pl.when((s <= f) & (f < NF - 1))
        def _():
            hop_right(tokens, s).wait_send()

        @pl.when((s >= f) & (f > 0))
        def _():
            hop_left(tokens, s).wait_send()


def fused(tokens, route_ids, route_weights, norm_gain, gate_master, up_master, down_master):
    NF, NT = lax.axis_size("fs"), lax.axis_size("tp")
    E, Dl, Fl = gate_master.shape
    T, Dq = tokens.shape
    K = route_ids.shape[1]
    capacity = max(2, 3 * T * K // (2 * E))
    C = -(-capacity // 8) * 8
    H = Dl // 2
    D = Dl * NF
    NX = NT // 2
    dma = pltpu.SemaphoreType.DMA
    vmem, hbm = pl.BlockSpec(memory_space=pltpu.VMEM), pl.BlockSpec(memory_space=pl.ANY)
    serve = jax.ShapeDtypeStruct((1, D, Fl), bf16)
    return pl.pallas_call(
        functools.partial(kernel, NF, NT, C),
        out_shape=(serve, serve, serve, jax.ShapeDtypeStruct((T, Dq), bf16)),
        in_specs=[vmem] * 4 + [hbm] * 3,
        out_specs=(hbm, hbm, hbm, vmem),
        scratch_shapes=[
            pltpu.VMEM((NF + 1, H, Fl), f32),
            pltpu.VMEM((NF + 1, H, Fl), f32),
            pltpu.VMEM((NF + 1, H, Fl), f32),
            pltpu.VMEM((Dl, Fl), f32),
            pltpu.VMEM((NF, T, Dq), bf16),
            pltpu.VMEM((NF, K, T), i32),
            pltpu.VMEM((NT, NF, C, Dq), bf16),
            pltpu.VMEM((NF, C, Fl), f32),
            pltpu.VMEM((NF, C, 2 * Fl), f32),
            pltpu.VMEM((NF, 2, C, T), bf16),
            pltpu.VMEM((NF, H, Fl), bf16),
            pltpu.VMEM((NF, H, 2 * Fl), bf16),
            pltpu.VMEM((D, Fl), bf16),
            pltpu.VMEM((D, 2 * Fl), bf16),
            pltpu.VMEM((NT, Dq, Fl), bf16),
            pltpu.VMEM((NT, NF, C, Fl), bf16),
            pltpu.VMEM((NF, C, Dq), bf16),
            pltpu.VMEM((NF, C, Dq), bf16),
            dma((3, NF + 1)),
            dma((NF,)), dma((NF,)),
            dma((2, NF)), dma((NF,)),
            dma((NT, NF)), dma((NX, NF)), dma((NT, NF)),
            dma((NF,)), dma((NF,)), dma((NF,)), dma((NF,)),
            dma((NF,)), dma((NF,)), dma((NF,)), dma((NF,)),
            dma((NT, 2)), dma((NT, 2)), dma(()),
            dma((NT, NF)), dma((NX, NF)), dma((NT, NF)),
            dma((NF,)), dma((NF,)),
            dma((3,)),
        ],
        compiler_params=pltpu.CompilerParams(
            collective_id=0, has_side_effects=True, vmem_limit_bytes=56 * 1024 * 1024
        ),
    )(
        tokens, route_ids.T, route_weights.T, norm_gain[None, :],
        gate_master, up_master, down_master,
    )


def solution(mesh):
    shape = mesh.shape
    fits = shape['grp'] == 2 and shape['tp'] % 2 == 0 and shape['fs'] == shape['tp'] <= 8
    body = fused if fits else local
    placed = (
        P(("grp", "fs"), "tp"),
        P(("grp", "fs"), None),
        P(("grp", "fs"), None),
        P("fs"),
        P(None, "fs", "tp"),
        P(None, "fs", "tp"),
        P(None, "fs", "tp"),
    )
    return jax.shard_map(
        body,
        mesh=mesh,
        in_specs=placed,
        out_specs=(
            P(("grp", "fs"), None, "tp"),
            P(("grp", "fs"), None, "tp"),
            P(("grp", "fs"), None, "tp"),
            P(("grp", "fs"), "tp"),
        ),
        check_vma=False,
    )
```

```python
import functools
import jax
import jax.numpy as jnp
from jax import lax
from jax.experimental import pallas as pl
from jax.experimental.pallas import tpu as pltpu
from jax.sharding import PartitionSpec as P

norm_epsilon = 1e-06


def slot_numbers(route_ids, experts, capacity):
    flat_ids = route_ids.reshape(-1)
    onehot = (flat_ids[:, None] == jnp.arange(experts, dtype=jnp.int32)[None, :]).astype(jnp.int32)
    before = jnp.cumsum(onehot, axis=0) - onehot
    position = jnp.sum(before * onehot, axis=1)
    return (flat_ids * capacity + position).reshape(route_ids.shape)


def local(tokens, route_ids, route_weights, norm_gain, gate_master, up_master, down_master):
    experts = gate_master.shape[0]
    shards = lax.axis_size("fs")
    columns = lax.axis_size("tp")
    per_device = experts // shards
    tok_rows = route_ids.shape[0]
    top_count = route_ids.shape[1]
    local_width = tokens.shape[1]
    model_width = local_width * columns
    capacity = max(2, 3 * tok_rows * top_count // (2 * experts))
    row_gain = norm_gain[None, :, None]
    gate_half = (gate_master * row_gain).astype(jnp.bfloat16)
    up_half = (up_master * row_gain).astype(jnp.bfloat16)
    down_half = down_master.astype(jnp.bfloat16)
    gate_serve, up_serve, down_serve = (
        lax.all_to_all(gate_half, "fs", split_axis=0, concat_axis=1, tiled=True),
        lax.all_to_all(up_half, "fs", split_axis=0, concat_axis=1, tiled=True),
        lax.all_to_all(down_half, "fs", split_axis=0, concat_axis=1, tiled=True),
    )
    slot_ids = slot_numbers(route_ids, experts, capacity)
    slot_range = jnp.arange(experts * capacity, dtype=jnp.int32)
    selects = [
        (slot_ids[:, rank_slot, None] == slot_range[None, :]).astype(jnp.bfloat16)
        for rank_slot in range(top_count)
    ]
    placing = selects[0]
    for extra in selects[1:]:
        placing = placing + extra
    local_values = tokens.astype(jnp.float32)
    squares = lax.psum(jnp.sum(local_values * local_values, axis=1), "tp")
    inverse = lax.rsqrt(squares / model_width + norm_epsilon)[:, None]
    normed = (local_values * inverse).astype(jnp.bfloat16)
    buffer = jnp.einsum("ts,td->sd", placing, normed, preferred_element_type=jnp.float32).astype(
        jnp.bfloat16
    )
    arrived = lax.all_to_all(
        buffer.reshape(shards, per_device * capacity, local_width),
        "fs",
        split_axis=0,
        concat_axis=0,
        tiled=True,
    )
    arrived = arrived.reshape(shards, per_device, capacity, local_width)
    partial_value = lax.all_gather(arrived, "tp", axis=3, tiled=True)
    gate_sum = jnp.einsum(
        "sxcd,xdf->xscf", partial_value, gate_serve, preferred_element_type=jnp.float32
    )
    up_sum = jnp.einsum(
        "sxcd,xdf->xscf", partial_value, up_serve, preferred_element_type=jnp.float32
    )
    hidden = (jax.nn.silu(gate_sum) * up_sum).astype(jnp.bfloat16)
    products = jnp.einsum("xdf,xscf->dsxc", down_serve, hidden, preferred_element_type=jnp.float32)
    summed = lax.psum_scatter(
        products.reshape(local_width * lax.axis_size("tp"), shards * per_device * capacity).astype(
            jnp.bfloat16
        ),
        "tp",
        scatter_dimension=0,
        tiled=True,
    )
    returned = lax.all_to_all(
        summed.reshape(local_width, shards, per_device * capacity),
        "fs",
        split_axis=1,
        concat_axis=1,
        tiled=True,
    )
    returned = returned.reshape(local_width, experts * capacity)
    combined = jnp.zeros((tok_rows, local_width), jnp.float32)
    for rank_slot in range(top_count):
        picked = jnp.einsum(
            "ts,ds->td", selects[rank_slot], returned, preferred_element_type=jnp.float32
        )
        combined = combined + route_weights[:, rank_slot : rank_slot + 1] * picked
    return (gate_serve, up_serve, down_serve, combined.astype(jnp.bfloat16))


MESH = pl.DeviceIdType.MESH
bf16, f32, i32 = jnp.bfloat16, jnp.float32, jnp.int32


def remote(src, dst, send, recv, to):
    return pltpu.make_async_remote_copy(
        src_ref=src, dst_ref=dst, send_sem=send, recv_sem=recv, device_id=to, device_id_type=MESH
    )


def kernel(
    NF, NT, C,
    tokens, ids_t, weights_t, gain, gm, um, dm,
    gate_o, up_o, down_o, moe_o,
    gmv, umv, dmv, gcol, toks, ids_all, xg, invs, acc, comb, sd, sgu, wd, wgu, wdq, hid, rs, ret,
    ld_sem, i_send, i_recv, c_send, c_recv, p_sib, p_x, p_recv,
    wd_send, wd_recv, wdy_send, wdy_recv, gu_send, gu_recv, guy_send, guy_recv,
    wq_send, wq_recv, wq_own, h_sib, h_x, h_recv, r_send, r_recv, o_sem,
):
    g, f, t = lax.axis_index("grp"), lax.axis_index("fs"), lax.axis_index("tp")
    NX = NT // 2
    chip, core = t // 2, lax.rem(t, 2)
    sib = chip * 2 + (1 - core)
    H, Fl = dmv.shape[1], dmv.shape[2]
    Dl = 2 * H
    T, Dq = tokens.shape
    D = NT * Dq
    ring = range(1, NF)

    def fs_at(k):
        return lax.rem(f + k + NF, NF)

    def rows(s, half):
        return pl.ds(pl.multiple_of(s * Dl + half * H, H), H)

    def both(s):
        return pl.ds(pl.multiple_of(s * Dl, Dl), Dl)

    halves = [(fs_at(k), g) for k in range(NF)] + [(f, 1 - g)]
    order = list(ring) + [0, NF]
    loads = {}
    for m, src, dst in ((0, gm, gmv), (1, um, umv), (2, dm, dmv)):
        for k in order:
            e, half = halves[k]
            cp = pltpu.make_async_copy(
                src.at[e, pl.ds(pl.multiple_of(half * H, H), H), :], dst.at[k], ld_sem.at[m, k]
            )
            cp.start()
            loads[m, k] = cp

    barrier = pltpu.get_barrier_semaphore()
    for k in ring:
        pl.semaphore_signal(barrier, inc=1, device_id={"fs": fs_at(k)}, device_id_type=MESH)
    for k in range(1, NT):
        pl.semaphore_signal(barrier, inc=1, device_id={"tp": lax.rem(t + k, NT)}, device_id_type=MESH)
    peer = {"grp": 1 - g}
    pl.semaphore_signal(barrier, inc=1, device_id=peer, device_id_type=MESH)

    earlier = (
        lax.broadcasted_iota(i32, (T, T), 0) < lax.broadcasted_iota(i32, (T, T), 1)
    ).astype(bf16)
    c_iota = lax.broadcasted_iota(i32, (C, T), 0).astype(f32)

    def slot_row(ids, e):
        member = jnp.max((ids == e).astype(f32), axis=0, keepdims=True)
        pos = jnp.dot(
            jnp.broadcast_to(member, (8, T)).astype(bf16), earlier, preferred_element_type=f32
        )
        return jnp.where(member > 0, pos[:1], -1.0)

    def place(s, ids, block):
        hot = (c_iota == slot_row(ids, f)).astype(bf16)
        xg[t, s] = jnp.dot(hot, block[...], preferred_element_type=f32).astype(bf16)

    pl.semaphore_wait(barrier, (NF - 1) + (NT - 1) + 1)

    waits = []

    def go(cp):
        cp.start()
        waits.append(cp)

    for k in ring:
        go(remote(ids_t, ids_all.at[f], i_send.at[k], i_recv.at[f], {"fs": fs_at(k)}))

    parts = 2 if T % 32 == 0 else 1
    Tp = T // parts

    def hop(src, b, p, way):
        cut = pl.ds(p * Tp, Tp)
        return remote(
            src.at[cut, :], toks.at[b, cut, :], c_send.at[(1 - way) // 2, b, p], c_recv.at[b, p], {"fs": f + way}
        )

    @pl.when(f < NF - 1)
    def _():
        for p in range(parts):
            hop(tokens, f, p, 1).start()

    @pl.when(f > 0)
    def _():
        for p in range(parts):
            hop(tokens, f, p, -1).start()

    def spread(buf, sems_sib, sems_x, sems_recv, s):
        for dx in range(1, NX):
            other = lax.rem(chip + dx, NX)
            remote(
                buf.at[t, s], buf.at[t, s], sems_x.at[dx, s], sems_recv.at[t, s],
                {"tp": other * 2 + core},
            ).start()
        remote(buf.at[t, s], buf.at[t, s], sems_sib.at[t, s], sems_recv.at[t, s], {"tp": sib}).start()

    def arrived(buf, sems_recv, q, s):
        remote(buf.at[q, s], buf.at[q, s], sems_recv.at[q, s], sems_recv.at[q, s], {"tp": sib}).wait_recv()

    def pass_on(buf, sems_sib, sems_recv, s):
        for dx in range(1, NX):
            q = lax.rem(chip + dx, NX) * 2 + core
            arrived(buf, sems_recv, q, s)
            remote(buf.at[q, s], buf.at[q, s], sems_sib.at[q, s], sems_recv.at[q, s], {"tp": sib}).start()

    def sib_arrived(buf, sems_recv, s):
        for dx in range(NX):
            arrived(buf, sems_recv, lax.rem(chip + dx, NX) * 2 + 1 - core, s)

    def spread_sent(buf, sems_sib, sems_x, s):
        for dx in range(1, NX):
            remote(buf.at[t, s], buf.at[t, s], sems_x.at[dx, s], sems_x.at[dx, s], {"tp": sib}).wait_send()
        for dx in range(NX):
            q = lax.rem(chip + dx, NX) * 2 + core
            remote(buf.at[q, s], buf.at[q, s], sems_sib.at[q, s], sems_sib.at[q, s], {"tp": sib}).wait_send()

    place(f, ids_t[...], tokens)
    spread(xg, p_sib, p_x, p_recv, f)

    gcol[...] = jnp.transpose(jnp.broadcast_to(gain[...], (Fl, Dl)))
    mine = pl.ds(pl.multiple_of(g * H, H), H)
    theirs = pl.ds(pl.multiple_of((1 - g) * H, H), H)
    for k in ring:
        loads[0, k].wait()
        loads[1, k].wait()
        sgu[k, :, :Fl] = (gmv[k] * gcol[mine, :]).astype(bf16)
        sgu[k, :, Fl:] = (umv[k] * gcol[mine, :]).astype(bf16)
    for k in ring:
        loads[2, k].wait()
        sd[k] = dmv[k].astype(bf16)

    def gu_copy(k, e):
        return remote(sgu.at[k], wgu.at[rows(f, g), :], gu_send.at[k], gu_recv.at[f], {"fs": e})

    def wd_copy(k, e):
        return remote(sd.at[k], wd.at[rows(f, g), :], wd_send.at[k], wd_recv.at[f], {"fs": e})

    def send_weights(at, way):
        reach = NF - 1 - at if way > 0 else at
        for make in (gu_copy, wd_copy):
            for dist in range(1, reach + 1):
                make(way * dist % NF, at + way * dist).start()

    for k, half, part in ((0, g, mine), (NF, 1 - g, theirs)):
        for m in range(3):
            loads[m, k].wait()
        wd[rows(f, half), :] = dmv[k].astype(bf16)
        wgu[rows(f, half), :Fl] = (gmv[k] * gcol[part, :]).astype(bf16)
        wgu[rows(f, half), Fl:] = (umv[k] * gcol[part, :]).astype(bf16)

    for k in ring:
        s = fs_at(k)
        remote(ids_t, ids_all.at[s], i_recv.at[s], i_recv.at[s], {"fs": s}).wait_recv()

    def take(b):
        place(b, ids_all[b], toks.at[b])
        spread(xg, p_sib, p_x, p_recv, b)

    for d in ring:
        for p in range(parts):
            @pl.when(f >= d)
            def _():
                hop(tokens, f - d, p, 1).wait_recv()

                @pl.when(f < NF - 1)
                def _():
                    hop(toks.at[f - d], f - d, p, 1).start()

            @pl.when(f + d < NF)
            def _():
                hop(tokens, f + d, p, -1).wait_recv()

                @pl.when(f > 0)
                def _():
                    hop(toks.at[f + d], f + d, p, -1).start()

        for at in range(NF):
            if max(at, NF - 1 - at) == d:
                @pl.when(f == at)
                def _():
                    send_weights(at, 1)
                    send_weights(at, -1)

        @pl.when(f >= d)
        def _():
            take(f - d)

        @pl.when(f + d < NF)
        def _():
            take(f + d)

        if d == 1:
            pass_on(xg, p_sib, p_recv, f)
        else:
            @pl.when(f >= d - 1)
            def _():
                pass_on(xg, p_sib, p_recv, f - d + 1)

            @pl.when(f + d - 1 < NF)
            def _():
                pass_on(xg, p_sib, p_recv, f + d - 1)

    by_distance = [sorted((s for s in range(NF) if s != a), key=lambda s: abs(s - a)) for a in range(NF)]

    def pick(column):
        out = jnp.int32(column[0])
        for a in range(1, NF):
            out = jnp.where(f == a, jnp.int32(column[a]), out)
        return out

    near = [pick([by_distance[a][i] for a in range(NF)]) for i in range(NF - 1)]

    def to_peer(buf, y_send, y_recv, recv, s):
        here = buf.at[rows(s, g), :]
        remote(here, here, recv.at[s], recv.at[s], {"fs": s}).wait_recv()
        remote(here, here, y_send.at[s], y_recv.at[s], peer).start()

    def from_peer(buf, y_recv, s):
        there = buf.at[rows(s, 1 - g), :]
        remote(there, there, y_recv.at[s], y_recv.at[s], peer).wait_recv()

    to_peer(wgu, guy_send, guy_recv, gu_recv, near[0])
    for d in (NF - 1,):
        @pl.when(f >= d)
        def _():
            pass_on(xg, p_sib, p_recv, f - d)

        @pl.when(f + d < NF)
        def _():
            pass_on(xg, p_sib, p_recv, f + d)
    for s in near[1:]:
        to_peer(wgu, guy_send, guy_recv, gu_recv, s)

    for e in range(NF):
        w_row = jnp.sum(jnp.where(ids_t[...] == e, weights_t[...], 0.0), axis=0, keepdims=True)
        w_at = jnp.where(c_iota == slot_row(ids_t[...], e), w_row, 0.0)
        high = w_at.astype(bf16)
        comb[e, 0] = high
        comb[e, 1] = (w_at - high.astype(f32)).astype(bf16)

    for k in range(NF):
        s = fs_at(k)
        sib_arrived(xg, p_recv, s)
        sq = jnp.zeros((C, 1), f32)
        for q in range(NT):
            xf = xg[q, s].astype(f32)
            sq = sq + jnp.sum(xf * xf, axis=1, keepdims=True)
        invs[s] = jnp.broadcast_to(lax.rsqrt(sq / D + norm_epsilon), (C, Fl))

    def partial_sums(q, first):
        w = wgu[both(q), :]
        for s in range(NF):
            part = jnp.dot(xg[q, s], w, preferred_element_type=f32)
            acc[s] = part if first else acc[s] + part

    def turned(s, half):
        part = pl.ds(pl.multiple_of(half * H, H), H)
        return remote(
            wd.at[rows(s, half), :], wdq.at[t, part, :], wq_send.at[s, half], wq_recv.at[t, half], {"tp": s}
        )

    own_q = pltpu.make_async_copy(wd.at[both(t), :], wdq.at[t], wq_own)

    def turn(s, half):
        @pl.when(s != t)
        def _():
            turned(s, half).start()

    turn(f, 0)
    turn(f, 1)
    partial_sums(f, True)
    for s in near:
        from_peer(wgu, guy_recv, s)
        partial_sums(s, False)
        to_peer(wd, wdy_send, wdy_recv, wd_recv, s)
        turn(s, g)
    outs = [
        pltpu.make_async_copy(wgu.at[:, :Fl], gate_o.at[0], o_sem.at[0]),
        pltpu.make_async_copy(wgu.at[:, Fl:], up_o.at[0], o_sem.at[1]),
        pltpu.make_async_copy(wd, down_o.at[0], o_sem.at[2]),
    ]
    outs[0].start()
    outs[1].start()

    far = near[::-1] + [f]
    for s in far:
        sums = acc[s]
        gate, up = sums[:, :Fl] * invs[s], sums[:, Fl:] * invs[s]
        hid[t, s] = (gate / (1.0 + jnp.exp(-gate)) * up).astype(bf16)
        spread(hid, h_sib, h_x, h_recv, s)

    for s in near:
        from_peer(wd, wdy_recv, s)
        turn(s, 1 - g)
    own_q.start()
    outs[2].start()
    for s in far:
        pass_on(hid, h_sib, h_recv, s)
    own_q.wait()
    for k in range(1, NT):
        q = lax.rem(t + k, NT)
        for half in range(2):
            part = wdq.at[q, half * H : (half + 1) * H, :]
            remote(part, part, wq_recv.at[q, half], wq_recv.at[q, half], {"tp": q}).wait_recv()
    for i, s in enumerate(far):
        sib_arrived(hid, h_recv, s)
        h = jnp.concatenate([hid[q, s] for q in range(NT)], axis=1)
        w = jnp.concatenate([wdq[q] for q in range(NT)], axis=1)
        y = lax.dot_general(h, w, (((1,), (1,)), ((), ())), preferred_element_type=f32).astype(bf16)
        if i == NF - 1:
            ret[f] = y
        else:
            rs[s] = y
            go(remote(rs.at[s], ret.at[f], r_send.at[s], r_recv.at[f], {"fs": s}))

    total = jnp.zeros((T, Dq), f32)
    for i, e in enumerate([f] + near):
        if i:
            remote(rs.at[e], ret.at[e], r_recv.at[e], r_recv.at[e], {"fs": e}).wait_recv()
        for term in range(2):
            total = total + lax.dot_general(
                comb[e, term], ret[e], (((0,), (0,)), ((), ())), preferred_element_type=f32
            )
    moe_o[...] = total.astype(bf16)

    for cp in outs:
        cp.wait()
    for cp in waits:
        cp.wait_send()
    for k in ring:
        s = fs_at(k)
        gu_copy(k, s).wait_send()
        wd_copy(k, s).wait_send()
        for buf, y_send in ((wgu, guy_send), (wd, wdy_send)):
            here = buf.at[rows(s, g), :]
            remote(here, here, y_send.at[s], y_send.at[s], peer).wait_send()
    for s in range(NF):
        @pl.when(s != t)
        def _():
            turned(s, 0).wait_send()
            turned(s, 1).wait_send()

        spread_sent(xg, p_sib, p_x, s)
        spread_sent(hid, h_sib, h_x, s)

        for p in range(parts):
            @pl.when((s <= f) & (f < NF - 1))
            def _():
                hop(tokens, s, p, 1).wait_send()

            @pl.when((s >= f) & (f > 0))
            def _():
                hop(tokens, s, p, -1).wait_send()


def fused(tokens, route_ids, route_weights, norm_gain, gate_master, up_master, down_master):
    NF, NT = lax.axis_size("fs"), lax.axis_size("tp")
    E, Dl, Fl = gate_master.shape
    T, Dq = tokens.shape
    K = route_ids.shape[1]
    capacity = max(2, 3 * T * K // (2 * E))
    C = -(-capacity // 8) * 8
    H = Dl // 2
    D = Dl * NF
    NX = NT // 2
    dma = pltpu.SemaphoreType.DMA
    vmem, hbm = pl.BlockSpec(memory_space=pltpu.VMEM), pl.BlockSpec(memory_space=pl.ANY)
    serve = jax.ShapeDtypeStruct((1, D, Fl), bf16)
    return pl.pallas_call(
        functools.partial(kernel, NF, NT, C),
        out_shape=(serve, serve, serve, jax.ShapeDtypeStruct((T, Dq), bf16)),
        in_specs=[vmem] * 4 + [hbm] * 3,
        out_specs=(hbm, hbm, hbm, vmem),
        scratch_shapes=[
            pltpu.VMEM((NF + 1, H, Fl), f32),
            pltpu.VMEM((NF + 1, H, Fl), f32),
            pltpu.VMEM((NF + 1, H, Fl), f32),
            pltpu.VMEM((Dl, Fl), f32),
            pltpu.VMEM((NF, T, Dq), bf16),
            pltpu.VMEM((NF, K, T), i32),
            pltpu.VMEM((NT, NF, C, Dq), bf16),
            pltpu.VMEM((NF, C, Fl), f32),
            pltpu.VMEM((NF, C, 2 * Fl), f32),
            pltpu.VMEM((NF, 2, C, T), bf16),
            pltpu.VMEM((NF, H, Fl), bf16),
            pltpu.VMEM((NF, H, 2 * Fl), bf16),
            pltpu.VMEM((D, Fl), bf16),
            pltpu.VMEM((D, 2 * Fl), bf16),
            pltpu.VMEM((NT, Dq, Fl), bf16),
            pltpu.VMEM((NT, NF, C, Fl), bf16),
            pltpu.VMEM((NF, C, Dq), bf16),
            pltpu.VMEM((NF, C, Dq), bf16),
            dma((3, NF + 1)),
            dma((NF,)), dma((NF,)),
            dma((2, NF, 2)), dma((NF, 2)),
            dma((NT, NF)), dma((NX, NF)), dma((NT, NF)),
            dma((NF,)), dma((NF,)), dma((NF,)), dma((NF,)),
            dma((NF,)), dma((NF,)), dma((NF,)), dma((NF,)),
            dma((NT, 2)), dma((NT, 2)), dma(()),
            dma((NT, NF)), dma((NX, NF)), dma((NT, NF)),
            dma((NF,)), dma((NF,)),
            dma((3,)),
        ],
        compiler_params=pltpu.CompilerParams(
            collective_id=0, has_side_effects=True, vmem_limit_bytes=56 * 1024 * 1024
        ),
    )(
        tokens, route_ids.T, route_weights.T, norm_gain[None, :],
        gate_master, up_master, down_master,
    )


def solution(mesh):
    shape = mesh.shape
    fits = shape['grp'] == 2 and shape['tp'] % 2 == 0 and shape['fs'] == shape['tp'] <= 8
    body = fused if fits else local
    placed = (
        P(("grp", "fs"), "tp"),
        P(("grp", "fs"), None),
        P(("grp", "fs"), None),
        P("fs"),
        P(None, "fs", "tp"),
        P(None, "fs", "tp"),
        P(None, "fs", "tp"),
    )
    return jax.shard_map(
        body,
        mesh=mesh,
        in_specs=placed,
        out_specs=(
            P(("grp", "fs"), None, "tp"),
            P(("grp", "fs"), None, "tp"),
            P(("grp", "fs"), None, "tp"),
            P(("grp", "fs"), "tp"),
        ),
        check_vma=False,
    )
```

```python
import functools
import jax
import jax.numpy as jnp
from jax import lax
from jax.experimental import pallas as pl
from jax.experimental.pallas import tpu as pltpu
from jax.sharding import PartitionSpec as P

norm_epsilon = 1e-06


def slot_numbers(route_ids, experts, capacity):
    flat_ids = route_ids.reshape(-1)
    onehot = (flat_ids[:, None] == jnp.arange(experts, dtype=jnp.int32)[None, :]).astype(jnp.int32)
    before = jnp.cumsum(onehot, axis=0) - onehot
    position = jnp.sum(before * onehot, axis=1)
    return (flat_ids * capacity + position).reshape(route_ids.shape)


def local(tokens, route_ids, route_weights, norm_gain, gate_master, up_master, down_master):
    experts = gate_master.shape[0]
    shards = lax.axis_size("fs")
    columns = lax.axis_size("tp")
    per_device = experts // shards
    tok_rows = route_ids.shape[0]
    top_count = route_ids.shape[1]
    local_width = tokens.shape[1]
    model_width = local_width * columns
    capacity = max(2, 3 * tok_rows * top_count // (2 * experts))
    row_gain = norm_gain[None, :, None]
    gate_half = (gate_master * row_gain).astype(jnp.bfloat16)
    up_half = (up_master * row_gain).astype(jnp.bfloat16)
    down_half = down_master.astype(jnp.bfloat16)
    gate_serve, up_serve, down_serve = (
        lax.all_to_all(gate_half, "fs", split_axis=0, concat_axis=1, tiled=True),
        lax.all_to_all(up_half, "fs", split_axis=0, concat_axis=1, tiled=True),
        lax.all_to_all(down_half, "fs", split_axis=0, concat_axis=1, tiled=True),
    )
    slot_ids = slot_numbers(route_ids, experts, capacity)
    slot_range = jnp.arange(experts * capacity, dtype=jnp.int32)
    selects = [
        (slot_ids[:, rank_slot, None] == slot_range[None, :]).astype(jnp.bfloat16)
        for rank_slot in range(top_count)
    ]
    placing = selects[0]
    for extra in selects[1:]:
        placing = placing + extra
    local_values = tokens.astype(jnp.float32)
    squares = lax.psum(jnp.sum(local_values * local_values, axis=1), "tp")
    inverse = lax.rsqrt(squares / model_width + norm_epsilon)[:, None]
    normed = (local_values * inverse).astype(jnp.bfloat16)
    buffer = jnp.einsum("ts,td->sd", placing, normed, preferred_element_type=jnp.float32).astype(
        jnp.bfloat16
    )
    arrived = lax.all_to_all(
        buffer.reshape(shards, per_device * capacity, local_width),
        "fs",
        split_axis=0,
        concat_axis=0,
        tiled=True,
    )
    arrived = arrived.reshape(shards, per_device, capacity, local_width)
    partial_value = lax.all_gather(arrived, "tp", axis=3, tiled=True)
    gate_sum = jnp.einsum(
        "sxcd,xdf->xscf", partial_value, gate_serve, preferred_element_type=jnp.float32
    )
    up_sum = jnp.einsum(
        "sxcd,xdf->xscf", partial_value, up_serve, preferred_element_type=jnp.float32
    )
    hidden = (jax.nn.silu(gate_sum) * up_sum).astype(jnp.bfloat16)
    products = jnp.einsum("xdf,xscf->dsxc", down_serve, hidden, preferred_element_type=jnp.float32)
    summed = lax.psum_scatter(
        products.reshape(local_width * lax.axis_size("tp"), shards * per_device * capacity).astype(
            jnp.bfloat16
        ),
        "tp",
        scatter_dimension=0,
        tiled=True,
    )
    returned = lax.all_to_all(
        summed.reshape(local_width, shards, per_device * capacity),
        "fs",
        split_axis=1,
        concat_axis=1,
        tiled=True,
    )
    returned = returned.reshape(local_width, experts * capacity)
    combined = jnp.zeros((tok_rows, local_width), jnp.float32)
    for rank_slot in range(top_count):
        picked = jnp.einsum(
            "ts,ds->td", selects[rank_slot], returned, preferred_element_type=jnp.float32
        )
        combined = combined + route_weights[:, rank_slot : rank_slot + 1] * picked
    return (gate_serve, up_serve, down_serve, combined.astype(jnp.bfloat16))


MESH = pl.DeviceIdType.MESH
bf16, f32, i32 = jnp.bfloat16, jnp.float32, jnp.int32


def remote(src, dst, send, recv, to):
    return pltpu.make_async_remote_copy(
        src_ref=src, dst_ref=dst, send_sem=send, recv_sem=recv, device_id=to, device_id_type=MESH
    )


def kernel(
    NF, NT, C,
    tokens, ids_t, weights_t, gain, gm, um, dm,
    gate_o, up_o, down_o, moe_o,
    gmv, umv, dmv, gcol, toks, ids_all, xg, invs, acc, comb, sd, sgu, wd, wgu, wdq, hid, rs, ret,
    ld_sem, i_send, i_recv, c_send, c_recv, p_sib, p_x, p_recv,
    wd_send, wd_recv, wdy_send, wdy_recv, gu_send, gu_recv, guy_send, guy_recv,
    wq_send, wq_recv, wq_own, h_sib, h_x, h_recv, r_send, r_recv, o_sem,
):
    g, f, t = lax.axis_index("grp"), lax.axis_index("fs"), lax.axis_index("tp")
    NX = NT // 2
    chip, core = t // 2, lax.rem(t, 2)
    sib = chip * 2 + (1 - core)
    H, Fl = dmv.shape[1], dmv.shape[2]
    Dl = 2 * H
    T, Dq = tokens.shape
    D = NT * Dq
    ring = range(1, NF)

    def fs_at(k):
        return lax.rem(f + k + NF, NF)

    def rows(s, half):
        return pl.ds(pl.multiple_of(s * Dl + half * H, H), H)

    def both(s):
        return pl.ds(pl.multiple_of(s * Dl, Dl), Dl)

    halves = [(fs_at(k), g) for k in range(NF)] + [(f, 1 - g)]
    order = list(ring) + [0, NF]
    loads = {}
    for m, src, dst in ((0, gm, gmv), (1, um, umv), (2, dm, dmv)):
        for k in order:
            e, half = halves[k]
            cp = pltpu.make_async_copy(
                src.at[e, pl.ds(pl.multiple_of(half * H, H), H), :], dst.at[k], ld_sem.at[m, k]
            )
            cp.start()
            loads[m, k] = cp

    barrier = pltpu.get_barrier_semaphore()
    for k in ring:
        pl.semaphore_signal(barrier, inc=1, device_id={"fs": fs_at(k)}, device_id_type=MESH)
    for k in range(1, NT):
        pl.semaphore_signal(barrier, inc=1, device_id={"tp": lax.rem(t + k, NT)}, device_id_type=MESH)
    peer = {"grp": 1 - g}
    pl.semaphore_signal(barrier, inc=1, device_id=peer, device_id_type=MESH)

    earlier = (
        lax.broadcasted_iota(i32, (T, T), 0) < lax.broadcasted_iota(i32, (T, T), 1)
    ).astype(bf16)
    c_iota = lax.broadcasted_iota(i32, (C, T), 0).astype(f32)

    def slot_row(ids, e):
        member = jnp.max((ids == e).astype(f32), axis=0, keepdims=True)
        pos = jnp.dot(
            jnp.broadcast_to(member, (8, T)).astype(bf16), earlier, preferred_element_type=f32
        )
        return jnp.where(member > 0, pos[:1], -1.0)

    def place(s, ids, block):
        hot = (c_iota == slot_row(ids, f)).astype(bf16)
        xg[t, s] = jnp.dot(hot, block[...], preferred_element_type=f32).astype(bf16)

    pl.semaphore_wait(barrier, (NF - 1) + (NT - 1) + 1)

    waits = []

    def go(cp):
        cp.start()
        waits.append(cp)

    for k in ring:
        go(remote(ids_t, ids_all.at[f], i_send.at[k], i_recv.at[f], {"fs": fs_at(k)}))

    parts = 2 if T % 32 == 0 else 1
    Tp = T // parts

    def hop(src, b, p, way):
        cut = pl.ds(p * Tp, Tp)
        return remote(
            src.at[cut, :], toks.at[b, cut, :], c_send.at[(1 - way) // 2, b, p], c_recv.at[b, p], {"fs": f + way}
        )

    @pl.when(f < NF - 1)
    def _():
        for p in range(parts):
            hop(tokens, f, p, 1).start()

    @pl.when(f > 0)
    def _():
        for p in range(parts):
            hop(tokens, f, p, -1).start()

    def spread(buf, sems_sib, sems_x, sems_recv, s):
        for dx in range(1, NX):
            other = lax.rem(chip + dx, NX)
            remote(
                buf.at[t, s], buf.at[t, s], sems_x.at[dx, s], sems_recv.at[t, s],
                {"tp": other * 2 + core},
            ).start()
        remote(buf.at[t, s], buf.at[t, s], sems_sib.at[t, s], sems_recv.at[t, s], {"tp": sib}).start()

    def arrived(buf, sems_recv, q, s):
        remote(buf.at[q, s], buf.at[q, s], sems_recv.at[q, s], sems_recv.at[q, s], {"tp": sib}).wait_recv()

    def pass_on(buf, sems_sib, sems_recv, s):
        for dx in range(1, NX):
            q = lax.rem(chip + dx, NX) * 2 + core
            arrived(buf, sems_recv, q, s)
            remote(buf.at[q, s], buf.at[q, s], sems_sib.at[q, s], sems_recv.at[q, s], {"tp": sib}).start()

    def sib_arrived(buf, sems_recv, s):
        for dx in range(NX):
            arrived(buf, sems_recv, lax.rem(chip + dx, NX) * 2 + 1 - core, s)

    def spread_sent(buf, sems_sib, sems_x, s):
        for dx in range(1, NX):
            remote(buf.at[t, s], buf.at[t, s], sems_x.at[dx, s], sems_x.at[dx, s], {"tp": sib}).wait_send()
        for dx in range(NX):
            q = lax.rem(chip + dx, NX) * 2 + core
            remote(buf.at[q, s], buf.at[q, s], sems_sib.at[q, s], sems_sib.at[q, s], {"tp": sib}).wait_send()

    place(f, ids_t[...], tokens)
    spread(xg, p_sib, p_x, p_recv, f)

    gcol[...] = jnp.transpose(jnp.broadcast_to(gain[...], (Fl, Dl)))
    mine = pl.ds(pl.multiple_of(g * H, H), H)
    theirs = pl.ds(pl.multiple_of((1 - g) * H, H), H)
    for k in ring:
        loads[0, k].wait()
        loads[1, k].wait()
        sgu[k, :, :Fl] = (gmv[k] * gcol[mine, :]).astype(bf16)
        sgu[k, :, Fl:] = (umv[k] * gcol[mine, :]).astype(bf16)
    for k in ring:
        loads[2, k].wait()
        sd[k] = dmv[k].astype(bf16)

    def gu_copy(k, e):
        return remote(sgu.at[k], wgu.at[rows(f, g), :], gu_send.at[k], gu_recv.at[f], {"fs": e})

    def wd_copy(k, e):
        return remote(sd.at[k], wd.at[rows(f, g), :], wd_send.at[k], wd_recv.at[f], {"fs": e})

    def send_weights(at, way):
        reach = NF - 1 - at if way > 0 else at
        for make in (gu_copy, wd_copy):
            for dist in range(1, reach + 1):
                make(way * dist % NF, at + way * dist).start()

    for k, half, part in ((0, g, mine), (NF, 1 - g, theirs)):
        for m in range(3):
            loads[m, k].wait()
        wd[rows(f, half), :] = dmv[k].astype(bf16)
        wgu[rows(f, half), :Fl] = (gmv[k] * gcol[part, :]).astype(bf16)
        wgu[rows(f, half), Fl:] = (umv[k] * gcol[part, :]).astype(bf16)

    for k in ring:
        s = fs_at(k)
        remote(ids_t, ids_all.at[s], i_recv.at[s], i_recv.at[s], {"fs": s}).wait_recv()

    def take(b):
        place(b, ids_all[b], toks.at[b])
        spread(xg, p_sib, p_x, p_recv, b)

    for d in ring:
        for p in range(parts):
            @pl.when(f >= d)
            def _():
                hop(tokens, f - d, p, 1).wait_recv()

                @pl.when(f < NF - 1)
                def _():
                    hop(toks.at[f - d], f - d, p, 1).start()

            @pl.when(f + d < NF)
            def _():
                hop(tokens, f + d, p, -1).wait_recv()

                @pl.when(f > 0)
                def _():
                    hop(toks.at[f + d], f + d, p, -1).start()

        for at in range(NF):
            if max(at, NF - 1 - at) == d:
                @pl.when(f == at)
                def _():
                    send_weights(at, 1)
                    send_weights(at, -1)

        @pl.when(f >= d)
        def _():
            take(f - d)

        @pl.when(f + d < NF)
        def _():
            take(f + d)

        if d == 1:
            pass_on(xg, p_sib, p_recv, f)
        else:
            @pl.when(f >= d - 1)
            def _():
                pass_on(xg, p_sib, p_recv, f - d + 1)

            @pl.when(f + d - 1 < NF)
            def _():
                pass_on(xg, p_sib, p_recv, f + d - 1)

    by_distance = [sorted((s for s in range(NF) if s != a), key=lambda s: abs(s - a)) for a in range(NF)]

    def pick(column):
        out = jnp.int32(column[0])
        for a in range(1, NF):
            out = jnp.where(f == a, jnp.int32(column[a]), out)
        return out

    near = [pick([by_distance[a][i] for a in range(NF)]) for i in range(NF - 1)]

    def to_peer(buf, y_send, y_recv, recv, s):
        here = buf.at[rows(s, g), :]
        remote(here, here, recv.at[s], recv.at[s], {"fs": s}).wait_recv()
        remote(here, here, y_send.at[s], y_recv.at[s], peer).start()

    def from_peer(buf, y_recv, s):
        there = buf.at[rows(s, 1 - g), :]
        remote(there, there, y_recv.at[s], y_recv.at[s], peer).wait_recv()

    to_peer(wgu, guy_send, guy_recv, gu_recv, near[0])
    for d in (NF - 1,):
        @pl.when(f >= d)
        def _():
            pass_on(xg, p_sib, p_recv, f - d)

        @pl.when(f + d < NF)
        def _():
            pass_on(xg, p_sib, p_recv, f + d)
    for s in near[1:]:
        to_peer(wgu, guy_send, guy_recv, gu_recv, s)

    for e in range(NF):
        w_row = jnp.sum(jnp.where(ids_t[...] == e, weights_t[...], 0.0), axis=0, keepdims=True)
        w_at = jnp.where(c_iota == slot_row(ids_t[...], e), w_row, 0.0)
        high = w_at.astype(bf16)
        comb[e, 0] = high
        comb[e, 1] = (w_at - high.astype(f32)).astype(bf16)

    for k in range(NF):
        s = fs_at(k)
        sib_arrived(xg, p_recv, s)
        sq = jnp.zeros((C, 1), f32)
        for q in range(NT):
            xf = xg[q, s].astype(f32)
            sq = sq + jnp.sum(xf * xf, axis=1, keepdims=True)
        invs[s] = jnp.broadcast_to(lax.rsqrt(sq / D + norm_epsilon), (C, Fl))

    def partial_sums(q, first):
        w = wgu[both(q), :]
        for s in range(NF):
            part = jnp.dot(xg[q, s], w, preferred_element_type=f32)
            acc[s] = part if first else acc[s] + part

    def turned(s, half):
        part = pl.ds(pl.multiple_of(half * H, H), H)
        return remote(
            wd.at[rows(s, half), :], wdq.at[t, part, :], wq_send.at[s, half], wq_recv.at[t, half], {"tp": s}
        )

    own_q = pltpu.make_async_copy(wd.at[both(t), :], wdq.at[t], wq_own)

    def turn(s, half):
        @pl.when(s != t)
        def _():
            turned(s, half).start()

    turn(f, 0)
    turn(f, 1)
    partial_sums(f, True)
    for s in near:
        from_peer(wgu, guy_recv, s)
        partial_sums(s, False)
        to_peer(wd, wdy_send, wdy_recv, wd_recv, s)
        turn(s, g)
    outs = [
        pltpu.make_async_copy(wgu.at[:, :Fl], gate_o.at[0], o_sem.at[0]),
        pltpu.make_async_copy(wgu.at[:, Fl:], up_o.at[0], o_sem.at[1]),
        pltpu.make_async_copy(wd, down_o.at[0], o_sem.at[2]),
    ]
    outs[0].start()
    outs[1].start()

    far = near[::-1] + [f]
    for s in far:
        sums = acc[s]
        gate, up = sums[:, :Fl] * invs[s], sums[:, Fl:] * invs[s]
        hid[t, s] = (gate / (1.0 + jnp.exp(-gate)) * up).astype(bf16)
        spread(hid, h_sib, h_x, h_recv, s)

    for s in near:
        from_peer(wd, wdy_recv, s)
        turn(s, 1 - g)
    own_q.start()
    outs[2].start()
    for s in far:
        pass_on(hid, h_sib, h_recv, s)
    own_q.wait()
    for k in range(1, NT):
        q = lax.rem(t + k, NT)
        for half in range(2):
            part = wdq.at[q, half * H : (half + 1) * H, :]
            remote(part, part, wq_recv.at[q, half], wq_recv.at[q, half], {"tp": q}).wait_recv()
    for i, s in enumerate(far):
        sib_arrived(hid, h_recv, s)
        h = jnp.concatenate([hid[q, s] for q in range(NT)], axis=1)
        w = jnp.concatenate([wdq[q] for q in range(NT)], axis=1)
        y = lax.dot_general(h, w, (((1,), (1,)), ((), ())), preferred_element_type=f32).astype(bf16)
        if i == NF - 1:
            ret[f] = y
        else:
            rs[s] = y
            go(remote(rs.at[s], ret.at[f], r_send.at[s], r_recv.at[f], {"fs": s}))

    total = jnp.zeros((T, Dq), f32)
    for i, e in enumerate([f] + near):
        if i:
            remote(rs.at[e], ret.at[e], r_recv.at[e], r_recv.at[e], {"fs": e}).wait_recv()
        for term in range(2):
            total = total + lax.dot_general(
                comb[e, term], ret[e], (((0,), (0,)), ((), ())), preferred_element_type=f32
            )
    moe_o[...] = total.astype(bf16)

    for cp in outs:
        cp.wait()
    for cp in waits:
        cp.wait_send()
    for k in ring:
        s = fs_at(k)
        gu_copy(k, s).wait_send()
        wd_copy(k, s).wait_send()
        for buf, y_send in ((wgu, guy_send), (wd, wdy_send)):
            here = buf.at[rows(s, g), :]
            remote(here, here, y_send.at[s], y_send.at[s], peer).wait_send()
    for s in range(NF):
        @pl.when(s != t)
        def _():
            turned(s, 0).wait_send()
            turned(s, 1).wait_send()

        spread_sent(xg, p_sib, p_x, s)
        spread_sent(hid, h_sib, h_x, s)

        for p in range(parts):
            @pl.when((s <= f) & (f < NF - 1))
            def _():
                hop(tokens, s, p, 1).wait_send()

            @pl.when((s >= f) & (f > 0))
            def _():
                hop(tokens, s, p, -1).wait_send()


def finish(n, pieces, *refs):
    ins, outs, stage, sems = refs[:n], refs[n : 2 * n], refs[2 * n : 3 * n], refs[3 * n]
    cuts = []
    for i, ref in enumerate(ins):
        size = ref.shape[-2] // pieces
        for p in range(pieces):
            at = (0,) * (len(ref.shape) - 2) + (pl.ds(p * size, size), slice(None))
            cuts.append((i, p, at))
    there = {}
    for i, p, at in cuts:
        there[i, p] = pltpu.make_async_copy(ins[i].at[at], stage[i].at[at], sems.at[0, i, p])
        there[i, p].start()
    back = []
    for i, p, at in cuts:
        there[i, p].wait()
        cp = pltpu.make_async_copy(stage[i].at[at], outs[i].at[at], sems.at[1, i, p])
        cp.start()
        back.append(cp)
    for cp in back:
        cp.wait()


def fused(tokens, route_ids, route_weights, norm_gain, gate_master, up_master, down_master):
    NF, NT = lax.axis_size("fs"), lax.axis_size("tp")
    E, Dl, Fl = gate_master.shape
    T, Dq = tokens.shape
    K = route_ids.shape[1]
    capacity = max(2, 3 * T * K // (2 * E))
    C = -(-capacity // 8) * 8
    H = Dl // 2
    D = Dl * NF
    NX = NT // 2
    dma = pltpu.SemaphoreType.DMA
    vmem, hbm = pl.BlockSpec(memory_space=pltpu.VMEM), pl.BlockSpec(memory_space=pl.ANY)
    serve = jax.ShapeDtypeStruct((1, D, Fl), bf16)
    done = pl.pallas_call(
        functools.partial(kernel, NF, NT, C),
        out_shape=(serve, serve, serve, jax.ShapeDtypeStruct((T, Dq), bf16)),
        in_specs=[vmem] * 4 + [hbm] * 3,
        out_specs=(hbm, hbm, hbm, vmem),
        scratch_shapes=[
            pltpu.VMEM((NF + 1, H, Fl), f32),
            pltpu.VMEM((NF + 1, H, Fl), f32),
            pltpu.VMEM((NF + 1, H, Fl), f32),
            pltpu.VMEM((Dl, Fl), f32),
            pltpu.VMEM((NF, T, Dq), bf16),
            pltpu.VMEM((NF, K, T), i32),
            pltpu.VMEM((NT, NF, C, Dq), bf16),
            pltpu.VMEM((NF, C, Fl), f32),
            pltpu.VMEM((NF, C, 2 * Fl), f32),
            pltpu.VMEM((NF, 2, C, T), bf16),
            pltpu.VMEM((NF, H, Fl), bf16),
            pltpu.VMEM((NF, H, 2 * Fl), bf16),
            pltpu.VMEM((D, Fl), bf16),
            pltpu.VMEM((D, 2 * Fl), bf16),
            pltpu.VMEM((NT, Dq, Fl), bf16),
            pltpu.VMEM((NT, NF, C, Fl), bf16),
            pltpu.VMEM((NF, C, Dq), bf16),
            pltpu.VMEM((NF, C, Dq), bf16),
            dma((3, NF + 1)),
            dma((NF,)), dma((NF,)),
            dma((2, NF, 2)), dma((NF, 2)),
            dma((NT, NF)), dma((NX, NF)), dma((NT, NF)),
            dma((NF,)), dma((NF,)), dma((NF,)), dma((NF,)),
            dma((NF,)), dma((NF,)), dma((NF,)), dma((NF,)),
            dma((NT, 2)), dma((NT, 2)), dma(()),
            dma((NT, NF)), dma((NX, NF)), dma((NT, NF)),
            dma((NF,)), dma((NF,)),
            dma((3,)),
        ],
        compiler_params=pltpu.CompilerParams(
            collective_id=0, has_side_effects=True, vmem_limit_bytes=56 * 1024 * 1024
        ),
    )(
        tokens, route_ids.T, route_weights.T, norm_gain[None, :],
        gate_master, up_master, down_master,
    )
    pieces = 2 if T % 32 == 0 else 1
    return pl.pallas_call(
        functools.partial(finish, len(done), pieces),
        out_shape=tuple(jax.ShapeDtypeStruct(a.shape, a.dtype) for a in done),
        in_specs=[hbm] * len(done),
        out_specs=(hbm,) * len(done),
        scratch_shapes=[pltpu.VMEM(a.shape, a.dtype) for a in done] + [dma((2, len(done), pieces))],
        compiler_params=pltpu.CompilerParams(vmem_limit_bytes=56 * 1024 * 1024),
    )(*done)


def solution(mesh):
    shape = mesh.shape
    fits = shape['grp'] == 2 and shape['tp'] % 2 == 0 and shape['fs'] == shape['tp'] <= 8
    body = fused if fits else local
    placed = (
        P(("grp", "fs"), "tp"),
        P(("grp", "fs"), None),
        P(("grp", "fs"), None),
        P("fs"),
        P(None, "fs", "tp"),
        P(None, "fs", "tp"),
        P(None, "fs", "tp"),
    )
    return jax.shard_map(
        body,
        mesh=mesh,
        in_specs=placed,
        out_specs=(
            P(("grp", "fs"), None, "tp"),
            P(("grp", "fs"), None, "tp"),
            P(("grp", "fs"), None, "tp"),
            P(("grp", "fs"), "tp"),
        ),
        check_vma=False,
    )
```

```python
import functools
import jax
import jax.numpy as jnp
from jax import lax
from jax.experimental import pallas as pl
from jax.experimental.pallas import tpu as pltpu
from jax.sharding import PartitionSpec as P

norm_epsilon = 1e-06


def slot_numbers(route_ids, experts, capacity):
    flat_ids = route_ids.reshape(-1)
    onehot = (flat_ids[:, None] == jnp.arange(experts, dtype=jnp.int32)[None, :]).astype(jnp.int32)
    before = jnp.cumsum(onehot, axis=0) - onehot
    position = jnp.sum(before * onehot, axis=1)
    return (flat_ids * capacity + position).reshape(route_ids.shape)


def local(tokens, route_ids, route_weights, norm_gain, gate_master, up_master, down_master):
    experts = gate_master.shape[0]
    shards = lax.axis_size("fs")
    columns = lax.axis_size("tp")
    per_device = experts // shards
    tok_rows = route_ids.shape[0]
    top_count = route_ids.shape[1]
    local_width = tokens.shape[1]
    model_width = local_width * columns
    capacity = max(2, 3 * tok_rows * top_count // (2 * experts))
    row_gain = norm_gain[None, :, None]
    gate_half = (gate_master * row_gain).astype(jnp.bfloat16)
    up_half = (up_master * row_gain).astype(jnp.bfloat16)
    down_half = down_master.astype(jnp.bfloat16)
    gate_serve, up_serve, down_serve = (
        lax.all_to_all(gate_half, "fs", split_axis=0, concat_axis=1, tiled=True),
        lax.all_to_all(up_half, "fs", split_axis=0, concat_axis=1, tiled=True),
        lax.all_to_all(down_half, "fs", split_axis=0, concat_axis=1, tiled=True),
    )
    slot_ids = slot_numbers(route_ids, experts, capacity)
    slot_range = jnp.arange(experts * capacity, dtype=jnp.int32)
    selects = [
        (slot_ids[:, rank_slot, None] == slot_range[None, :]).astype(jnp.bfloat16)
        for rank_slot in range(top_count)
    ]
    placing = selects[0]
    for extra in selects[1:]:
        placing = placing + extra
    local_values = tokens.astype(jnp.float32)
    squares = lax.psum(jnp.sum(local_values * local_values, axis=1), "tp")
    inverse = lax.rsqrt(squares / model_width + norm_epsilon)[:, None]
    normed = (local_values * inverse).astype(jnp.bfloat16)
    buffer = jnp.einsum("ts,td->sd", placing, normed, preferred_element_type=jnp.float32).astype(
        jnp.bfloat16
    )
    arrived = lax.all_to_all(
        buffer.reshape(shards, per_device * capacity, local_width),
        "fs",
        split_axis=0,
        concat_axis=0,
        tiled=True,
    )
    arrived = arrived.reshape(shards, per_device, capacity, local_width)
    partial_value = lax.all_gather(arrived, "tp", axis=3, tiled=True)
    gate_sum = jnp.einsum(
        "sxcd,xdf->xscf", partial_value, gate_serve, preferred_element_type=jnp.float32
    )
    up_sum = jnp.einsum(
        "sxcd,xdf->xscf", partial_value, up_serve, preferred_element_type=jnp.float32
    )
    hidden = (jax.nn.silu(gate_sum) * up_sum).astype(jnp.bfloat16)
    products = jnp.einsum("xdf,xscf->dsxc", down_serve, hidden, preferred_element_type=jnp.float32)
    summed = lax.psum_scatter(
        products.reshape(local_width * lax.axis_size("tp"), shards * per_device * capacity).astype(
            jnp.bfloat16
        ),
        "tp",
        scatter_dimension=0,
        tiled=True,
    )
    returned = lax.all_to_all(
        summed.reshape(local_width, shards, per_device * capacity),
        "fs",
        split_axis=1,
        concat_axis=1,
        tiled=True,
    )
    returned = returned.reshape(local_width, experts * capacity)
    combined = jnp.zeros((tok_rows, local_width), jnp.float32)
    for rank_slot in range(top_count):
        picked = jnp.einsum(
            "ts,ds->td", selects[rank_slot], returned, preferred_element_type=jnp.float32
        )
        combined = combined + route_weights[:, rank_slot : rank_slot + 1] * picked
    return (gate_serve, up_serve, down_serve, combined.astype(jnp.bfloat16))


MESH = pl.DeviceIdType.MESH
bf16, f32, i32 = jnp.bfloat16, jnp.float32, jnp.int32


def remote(src, dst, send, recv, to):
    return pltpu.make_async_remote_copy(
        src_ref=src, dst_ref=dst, send_sem=send, recv_sem=recv, device_id=to, device_id_type=MESH
    )


def kernel(
    NF, NT, C,
    tokens, ids_t, weights_t, gain, gm, um, dm,
    gate_o, up_o, down_o, moe_o,
    gmv, umv, dmv, gcol, toks, ids_all, xg, invs, acc, comb, sd, sgu, wd, wgu, wdq, hid, rs, ret,
    ld_sem, i_send, i_recv, c_send, c_recv, p_sib, p_x, p_recv,
    wd_send, wd_recv, wdy_send, wdy_recv, gu_send, gu_recv, guy_send, guy_recv,
    wq_send, wq_recv, wq_own, h_sib, h_x, h_recv, r_send, r_recv, o_sem,
):
    g, f, t = lax.axis_index("grp"), lax.axis_index("fs"), lax.axis_index("tp")
    NX = NT // 2
    chip, core = t // 2, lax.rem(t, 2)
    sib = chip * 2 + (1 - core)
    H, Fl = dmv.shape[1], dmv.shape[2]
    Dl = 2 * H
    T, Dq = tokens.shape
    D = NT * Dq
    ring = range(1, NF)

    def fs_at(k):
        return lax.rem(f + k + NF, NF)

    def rows(s, half):
        return pl.ds(pl.multiple_of(s * Dl + half * H, H), H)

    def both(s):
        return pl.ds(pl.multiple_of(s * Dl, Dl), Dl)

    halves = [(fs_at(k), g) for k in range(NF)] + [(f, 1 - g)]
    order = list(ring) + [0, NF]
    loads = {}
    for m, src, dst in ((0, gm, gmv), (1, um, umv), (2, dm, dmv)):
        for k in order:
            e, half = halves[k]
            cp = pltpu.make_async_copy(
                src.at[e, pl.ds(pl.multiple_of(half * H, H), H), :], dst.at[k], ld_sem.at[m, k]
            )
            cp.start()
            loads[m, k] = cp

    barrier = pltpu.get_barrier_semaphore()
    for k in ring:
        pl.semaphore_signal(barrier, inc=1, device_id={"fs": fs_at(k)}, device_id_type=MESH)
    for k in range(1, NT):
        pl.semaphore_signal(barrier, inc=1, device_id={"tp": lax.rem(t + k, NT)}, device_id_type=MESH)
    peer = {"grp": 1 - g}
    pl.semaphore_signal(barrier, inc=1, device_id=peer, device_id_type=MESH)

    earlier = (
        lax.broadcasted_iota(i32, (T, T), 0) < lax.broadcasted_iota(i32, (T, T), 1)
    ).astype(bf16)
    c_iota = lax.broadcasted_iota(i32, (C, T), 0).astype(f32)

    def slot_row(ids, e):
        member = jnp.max((ids == e).astype(f32), axis=0, keepdims=True)
        pos = jnp.dot(
            jnp.broadcast_to(member, (8, T)).astype(bf16), earlier, preferred_element_type=f32
        )
        return jnp.where(member > 0, pos[:1], -1.0)

    def place(s, ids, block):
        hot = (c_iota == slot_row(ids, f)).astype(bf16)
        xg[t, s] = jnp.dot(hot, block[...], preferred_element_type=f32).astype(bf16)

    pl.semaphore_wait(barrier, (NF - 1) + (NT - 1) + 1)

    waits = []

    def go(cp):
        cp.start()
        waits.append(cp)

    for k in ring:
        go(remote(ids_t, ids_all.at[f], i_send.at[k], i_recv.at[f], {"fs": fs_at(k)}))

    parts = 2 if T % 32 == 0 else 1
    Tp = T // parts

    def hop(src, b, p, way):
        cut = pl.ds(p * Tp, Tp)
        return remote(
            src.at[cut, :], toks.at[b, cut, :], c_send.at[(1 - way) // 2, b, p], c_recv.at[b, p], {"fs": f + way}
        )

    @pl.when(f < NF - 1)
    def _():
        for p in range(parts):
            hop(tokens, f, p, 1).start()

    @pl.when(f > 0)
    def _():
        for p in range(parts):
            hop(tokens, f, p, -1).start()

    def spread(buf, sems_sib, sems_x, sems_recv, s):
        for dx in range(1, NX):
            other = lax.rem(chip + dx, NX)
            remote(
                buf.at[t, s], buf.at[t, s], sems_x.at[dx, s], sems_recv.at[t, s],
                {"tp": other * 2 + core},
            ).start()
        remote(buf.at[t, s], buf.at[t, s], sems_sib.at[t, s], sems_recv.at[t, s], {"tp": sib}).start()

    def arrived(buf, sems_recv, q, s):
        remote(buf.at[q, s], buf.at[q, s], sems_recv.at[q, s], sems_recv.at[q, s], {"tp": sib}).wait_recv()

    def pass_on(buf, sems_sib, sems_recv, s):
        for dx in range(1, NX):
            q = lax.rem(chip + dx, NX) * 2 + core
            arrived(buf, sems_recv, q, s)
            remote(buf.at[q, s], buf.at[q, s], sems_sib.at[q, s], sems_recv.at[q, s], {"tp": sib}).start()

    def sib_arrived(buf, sems_recv, s):
        for dx in range(NX):
            arrived(buf, sems_recv, lax.rem(chip + dx, NX) * 2 + 1 - core, s)

    def spread_sent(buf, sems_sib, sems_x, s):
        for dx in range(1, NX):
            remote(buf.at[t, s], buf.at[t, s], sems_x.at[dx, s], sems_x.at[dx, s], {"tp": sib}).wait_send()
        for dx in range(NX):
            q = lax.rem(chip + dx, NX) * 2 + core
            remote(buf.at[q, s], buf.at[q, s], sems_sib.at[q, s], sems_sib.at[q, s], {"tp": sib}).wait_send()

    place(f, ids_t[...], tokens)
    spread(xg, p_sib, p_x, p_recv, f)

    gcol[...] = jnp.transpose(jnp.broadcast_to(gain[...], (Fl, Dl)))
    mine = pl.ds(pl.multiple_of(g * H, H), H)
    theirs = pl.ds(pl.multiple_of((1 - g) * H, H), H)
    for k in ring:
        loads[0, k].wait()
        loads[1, k].wait()
        sgu[k, :, :Fl] = (gmv[k] * gcol[mine, :]).astype(bf16)
        sgu[k, :, Fl:] = (umv[k] * gcol[mine, :]).astype(bf16)
    for k in ring:
        loads[2, k].wait()
        sd[k] = dmv[k].astype(bf16)

    def gu_copy(k, e):
        return remote(sgu.at[k], wgu.at[rows(f, g), :], gu_send.at[k], gu_recv.at[f], {"fs": e})

    def wd_copy(k, e):
        return remote(sd.at[k], wd.at[rows(f, g), :], wd_send.at[k], wd_recv.at[f], {"fs": e})

    def send_weights(at, way):
        reach = NF - 1 - at if way > 0 else at
        for make in (gu_copy, wd_copy):
            for dist in range(1, reach + 1):
                make(way * dist % NF, at + way * dist).start()

    for k, half, part in ((0, g, mine), (NF, 1 - g, theirs)):
        for m in range(3):
            loads[m, k].wait()
        wd[rows(f, half), :] = dmv[k].astype(bf16)
        wgu[rows(f, half), :Fl] = (gmv[k] * gcol[part, :]).astype(bf16)
        wgu[rows(f, half), Fl:] = (umv[k] * gcol[part, :]).astype(bf16)

    for k in ring:
        s = fs_at(k)
        remote(ids_t, ids_all.at[s], i_recv.at[s], i_recv.at[s], {"fs": s}).wait_recv()

    def take(b):
        place(b, ids_all[b], toks.at[b])
        spread(xg, p_sib, p_x, p_recv, b)

    for d in ring:
        for p in range(parts):
            @pl.when(f >= d)
            def _():
                hop(tokens, f - d, p, 1).wait_recv()

                @pl.when(f < NF - 1)
                def _():
                    hop(toks.at[f - d], f - d, p, 1).start()

            @pl.when(f + d < NF)
            def _():
                hop(tokens, f + d, p, -1).wait_recv()

                @pl.when(f > 0)
                def _():
                    hop(toks.at[f + d], f + d, p, -1).start()

        for at in range(NF):
            if max(at, NF - 1 - at) == d:
                @pl.when(f == at)
                def _():
                    send_weights(at, 1)
                    send_weights(at, -1)

        @pl.when(f >= d)
        def _():
            take(f - d)

        @pl.when(f + d < NF)
        def _():
            take(f + d)

        if d == 1:
            pass_on(xg, p_sib, p_recv, f)
        else:
            @pl.when(f >= d - 1)
            def _():
                pass_on(xg, p_sib, p_recv, f - d + 1)

            @pl.when(f + d - 1 < NF)
            def _():
                pass_on(xg, p_sib, p_recv, f + d - 1)

    by_distance = [sorted((s for s in range(NF) if s != a), key=lambda s: abs(s - a)) for a in range(NF)]

    def pick(column):
        out = jnp.int32(column[0])
        for a in range(1, NF):
            out = jnp.where(f == a, jnp.int32(column[a]), out)
        return out

    near = [pick([by_distance[a][i] for a in range(NF)]) for i in range(NF - 1)]

    def to_peer(buf, y_send, y_recv, recv, s):
        here = buf.at[rows(s, g), :]
        remote(here, here, recv.at[s], recv.at[s], {"fs": s}).wait_recv()
        remote(here, here, y_send.at[s], y_recv.at[s], peer).start()

    def from_peer(buf, y_recv, s):
        there = buf.at[rows(s, 1 - g), :]
        remote(there, there, y_recv.at[s], y_recv.at[s], peer).wait_recv()

    to_peer(wgu, guy_send, guy_recv, gu_recv, near[0])
    for d in (NF - 1,):
        @pl.when(f >= d)
        def _():
            pass_on(xg, p_sib, p_recv, f - d)

        @pl.when(f + d < NF)
        def _():
            pass_on(xg, p_sib, p_recv, f + d)
    for s in near[1:]:
        to_peer(wgu, guy_send, guy_recv, gu_recv, s)

    for e in range(NF):
        w_row = jnp.sum(jnp.where(ids_t[...] == e, weights_t[...], 0.0), axis=0, keepdims=True)
        w_at = jnp.where(c_iota == slot_row(ids_t[...], e), w_row, 0.0)
        high = w_at.astype(bf16)
        comb[e, 0] = high
        comb[e, 1] = (w_at - high.astype(f32)).astype(bf16)

    for k in range(NF):
        s = fs_at(k)
        sib_arrived(xg, p_recv, s)
        sq = jnp.zeros((C, 1), f32)
        for q in range(NT):
            xf = xg[q, s].astype(f32)
            sq = sq + jnp.sum(xf * xf, axis=1, keepdims=True)
        invs[s] = jnp.broadcast_to(lax.rsqrt(sq / D + norm_epsilon), (C, Fl))

    def partial_sums(q, first):
        w = wgu[both(q), :]
        for s in range(NF):
            part = jnp.dot(xg[q, s], w, preferred_element_type=f32)
            acc[s] = part if first else acc[s] + part

    def turned(s, half):
        part = pl.ds(pl.multiple_of(half * H, H), H)
        return remote(
            wd.at[rows(s, half), :], wdq.at[t, part, :], wq_send.at[s, half], wq_recv.at[t, half], {"tp": s}
        )

    own_q = pltpu.make_async_copy(wd.at[both(t), :], wdq.at[t], wq_own)

    def turn(s, half):
        @pl.when(s != t)
        def _():
            turned(s, half).start()

    turn(f, 0)
    turn(f, 1)
    partial_sums(f, True)
    for s in near:
        from_peer(wgu, guy_recv, s)
        partial_sums(s, False)
        if s is not near[-1]:
            to_peer(wd, wdy_send, wdy_recv, wd_recv, s)
            turn(s, g)
    outs = [
        pltpu.make_async_copy(wgu.at[:, :Fl], gate_o.at[0], o_sem.at[0]),
        pltpu.make_async_copy(wgu.at[:, Fl:], up_o.at[0], o_sem.at[1]),
        pltpu.make_async_copy(wd, down_o.at[0], o_sem.at[2]),
    ]
    outs[0].start()
    outs[1].start()

    far = near[::-1] + [f]
    for s in far:
        sums = acc[s]
        gate, up = sums[:, :Fl] * invs[s], sums[:, Fl:] * invs[s]
        hid[t, s] = (gate / (1.0 + jnp.exp(-gate)) * up).astype(bf16)
        spread(hid, h_sib, h_x, h_recv, s)

    to_peer(wd, wdy_send, wdy_recv, wd_recv, near[-1])
    turn(near[-1], g)
    for s in near:
        from_peer(wd, wdy_recv, s)
        turn(s, 1 - g)
    own_q.start()
    outs[2].start()
    for s in far:
        pass_on(hid, h_sib, h_recv, s)
    own_q.wait()
    for k in range(1, NT):
        q = lax.rem(t + k, NT)
        for half in range(2):
            part = wdq.at[q, half * H : (half + 1) * H, :]
            remote(part, part, wq_recv.at[q, half], wq_recv.at[q, half], {"tp": q}).wait_recv()
    for i, s in enumerate(far):
        sib_arrived(hid, h_recv, s)
        h = jnp.concatenate([hid[q, s] for q in range(NT)], axis=1)
        w = jnp.concatenate([wdq[q] for q in range(NT)], axis=1)
        y = lax.dot_general(h, w, (((1,), (1,)), ((), ())), preferred_element_type=f32).astype(bf16)
        if i == NF - 1:
            ret[f] = y
        else:
            rs[s] = y
            go(remote(rs.at[s], ret.at[f], r_send.at[s], r_recv.at[f], {"fs": s}))

    total = jnp.zeros((T, Dq), f32)
    for i, e in enumerate([f] + near):
        if i:
            remote(rs.at[e], ret.at[e], r_recv.at[e], r_recv.at[e], {"fs": e}).wait_recv()
        for term in range(2):
            total = total + lax.dot_general(
                comb[e, term], ret[e], (((0,), (0,)), ((), ())), preferred_element_type=f32
            )
    moe_o[...] = total.astype(bf16)

    for cp in outs:
        cp.wait()
    for cp in waits:
        cp.wait_send()
    for k in ring:
        s = fs_at(k)
        gu_copy(k, s).wait_send()
        wd_copy(k, s).wait_send()
        for buf, y_send in ((wgu, guy_send), (wd, wdy_send)):
            here = buf.at[rows(s, g), :]
            remote(here, here, y_send.at[s], y_send.at[s], peer).wait_send()
    for s in range(NF):
        @pl.when(s != t)
        def _():
            turned(s, 0).wait_send()
            turned(s, 1).wait_send()

        spread_sent(xg, p_sib, p_x, s)
        spread_sent(hid, h_sib, h_x, s)

        for p in range(parts):
            @pl.when((s <= f) & (f < NF - 1))
            def _():
                hop(tokens, s, p, 1).wait_send()

            @pl.when((s >= f) & (f > 0))
            def _():
                hop(tokens, s, p, -1).wait_send()


def finish(n, pieces, *refs):
    ins, outs, stage, sems = refs[:n], refs[n : 2 * n], refs[2 * n : 3 * n], refs[3 * n]
    cuts = []
    for i, ref in enumerate(ins):
        size = ref.shape[-2] // pieces
        for p in range(pieces):
            at = (0,) * (len(ref.shape) - 2) + (pl.ds(p * size, size), slice(None))
            cuts.append((i, p, at))
    there = {}
    for i, p, at in cuts:
        there[i, p] = pltpu.make_async_copy(ins[i].at[at], stage[i].at[at], sems.at[0, i, p])
        there[i, p].start()
    back = []
    for i, p, at in cuts:
        there[i, p].wait()
        cp = pltpu.make_async_copy(stage[i].at[at], outs[i].at[at], sems.at[1, i, p])
        cp.start()
        back.append(cp)
    for cp in back:
        cp.wait()


def fused(tokens, route_ids, route_weights, norm_gain, gate_master, up_master, down_master):
    NF, NT = lax.axis_size("fs"), lax.axis_size("tp")
    E, Dl, Fl = gate_master.shape
    T, Dq = tokens.shape
    K = route_ids.shape[1]
    capacity = max(2, 3 * T * K // (2 * E))
    C = -(-capacity // 8) * 8
    H = Dl // 2
    D = Dl * NF
    NX = NT // 2
    dma = pltpu.SemaphoreType.DMA
    vmem, hbm = pl.BlockSpec(memory_space=pltpu.VMEM), pl.BlockSpec(memory_space=pl.ANY)
    serve = jax.ShapeDtypeStruct((1, D, Fl), bf16)
    done = pl.pallas_call(
        functools.partial(kernel, NF, NT, C),
        out_shape=(serve, serve, serve, jax.ShapeDtypeStruct((T, Dq), bf16)),
        in_specs=[vmem] * 4 + [hbm] * 3,
        out_specs=(hbm, hbm, hbm, vmem),
        scratch_shapes=[
            pltpu.VMEM((NF + 1, H, Fl), f32),
            pltpu.VMEM((NF + 1, H, Fl), f32),
            pltpu.VMEM((NF + 1, H, Fl), f32),
            pltpu.VMEM((Dl, Fl), f32),
            pltpu.VMEM((NF, T, Dq), bf16),
            pltpu.VMEM((NF, K, T), i32),
            pltpu.VMEM((NT, NF, C, Dq), bf16),
            pltpu.VMEM((NF, C, Fl), f32),
            pltpu.VMEM((NF, C, 2 * Fl), f32),
            pltpu.VMEM((NF, 2, C, T), bf16),
            pltpu.VMEM((NF, H, Fl), bf16),
            pltpu.VMEM((NF, H, 2 * Fl), bf16),
            pltpu.VMEM((D, Fl), bf16),
            pltpu.VMEM((D, 2 * Fl), bf16),
            pltpu.VMEM((NT, Dq, Fl), bf16),
            pltpu.VMEM((NT, NF, C, Fl), bf16),
            pltpu.VMEM((NF, C, Dq), bf16),
            pltpu.VMEM((NF, C, Dq), bf16),
            dma((3, NF + 1)),
            dma((NF,)), dma((NF,)),
            dma((2, NF, 2)), dma((NF, 2)),
            dma((NT, NF)), dma((NX, NF)), dma((NT, NF)),
            dma((NF,)), dma((NF,)), dma((NF,)), dma((NF,)),
            dma((NF,)), dma((NF,)), dma((NF,)), dma((NF,)),
            dma((NT, 2)), dma((NT, 2)), dma(()),
            dma((NT, NF)), dma((NX, NF)), dma((NT, NF)),
            dma((NF,)), dma((NF,)),
            dma((3,)),
        ],
        compiler_params=pltpu.CompilerParams(
            collective_id=0, has_side_effects=True, vmem_limit_bytes=56 * 1024 * 1024
        ),
    )(
        tokens, route_ids.T, route_weights.T, norm_gain[None, :],
        gate_master, up_master, down_master,
    )
    pieces = 2 if T % 32 == 0 else 1
    return pl.pallas_call(
        functools.partial(finish, len(done), pieces),
        out_shape=tuple(jax.ShapeDtypeStruct(a.shape, a.dtype) for a in done),
        in_specs=[hbm] * len(done),
        out_specs=(hbm,) * len(done),
        scratch_shapes=[pltpu.VMEM(a.shape, a.dtype) for a in done] + [dma((2, len(done), pieces))],
        compiler_params=pltpu.CompilerParams(vmem_limit_bytes=56 * 1024 * 1024),
    )(*done)


def solution(mesh):
    shape = mesh.shape
    fits = shape['grp'] == 2 and shape['tp'] % 2 == 0 and shape['fs'] == shape['tp'] <= 8
    body = fused if fits else local
    placed = (
        P(("grp", "fs"), "tp"),
        P(("grp", "fs"), None),
        P(("grp", "fs"), None),
        P("fs"),
        P(None, "fs", "tp"),
        P(None, "fs", "tp"),
        P(None, "fs", "tp"),
    )
    return jax.shard_map(
        body,
        mesh=mesh,
        in_specs=placed,
        out_specs=(
            P(("grp", "fs"), None, "tp"),
            P(("grp", "fs"), None, "tp"),
            P(("grp", "fs"), None, "tp"),
            P(("grp", "fs"), "tp"),
        ),
        check_vma=False,
    )
```
